256 devices in a mesh: ep: 128 (over z, y, x), tp: 2 (over core).
Axes of the slice: x: 4, y: 4, z: 8, core: 2. Of those that a mesh axis runs over, the one named last changes fastest.
Arguments:
- tokens: bfloat16 [8192, 1024], P('ep', 'tp'), may hold values from -6 to 6
- norm_gain: float32 [1024], P('tp'), may hold values from 0.1 to 1.9
- routing: int32 [8192, 2], P('ep'), may hold values from 0 to 255, as said below
- route_weight: float32 [8192, 2], P('ep'), may hold values from 0.25 to 1
- w_gate: bfloat16 [256, 1024, 512], P('ep', None, 'tp'), may hold values from -0.1875 to 0.1875
- w_up: bfloat16 [256, 1024, 512], P('ep', None, 'tp'), may hold values from -0.1875 to 0.1875
- w_down: bfloat16 [256, 512, 1024], P('ep', None, 'tp'), may hold values from -0.25 to 0.25
Outputs:
- mixed: bfloat16 [8192, 1024], P('ep', 'tp')
The draws below stay inside these ranges and needn't reach their ends.
Inputs may be any that keep to these rules, and one draw needn't show every extreme that they name: `routing`: each row names 2 different experts, all in the same group of 8 consecutive expert numbers. Among the rows of one device (aligned blocks of 64 rows) no expert is named more than 8 times, and in every block some expert is named exactly 8 times.
All inputs are finite; a program needn't handle non-finite values.
Results may differ from the reference program's by a relative error of at most 0.0015.
Values may be sent and summed in bfloat16 or wider, within the bound.
No kernel may reach another device: no remote copies, remote signals or barrier semaphores. Data moves between devices by JAX's collectives and lax.ppermute only.
A program may use at most 64 MiB of HBM per device.

```python
import jax
import jax.numpy as jnp
from jax import lax

D = 1024
FFE = 512
TOP_K = 2
GROUP_EXP = 8
EXP_DEV = 2
CAP = 8
TOK_DEV = 64
EXPERTS = 256
TOKENS = 8192


def route_table(key):
    blocks = TOKENS // TOK_DEV
    groups = EXPERTS // GROUP_EXP
    semi_cluster = GROUP_EXP // 2
    opening_tally = EXPERTS // 2
    cell_count = TOK_DEV // CAP
    pop_key = jax.random.fold_in(key, 11)
    group_scores = jax.random.randint(pop_key, (groups,), 0, 1 << 20) * groups + jnp.arange(groups)
    ranking = jnp.argsort(jnp.argsort(group_scores))
    favoured_specialist = ranking < max(1, groups // 4)
    extra_cluster = jnp.where(favoured_specialist, 400, 0)
    base_key = jax.random.fold_in(key, 23)

    def one_block(block_id):
        block_key = jax.random.fold_in(base_key, block_id)
        perm_key, rating_seed, seat_key, flip_key = jax.random.split(block_key, 4)
        raw = jax.random.randint(perm_key, (groups, GROUP_EXP), 0, 1 << 20) * GROUP_EXP + jnp.arange(GROUP_EXP)[None, :]
        local_perm = jnp.argsort(raw, axis=1)
        pair_table = (jnp.arange(groups)[:, None] * GROUP_EXP + local_perm).reshape(opening_tally, 2)
        position = jnp.argsort(pair_table.reshape(-1))
        slot_of = position // 2
        forward = (block_id + blocks // 2) % blocks * EXP_DEV
        previous = (block_id + blocks - 1) % blocks * EXP_DEV
        opening_labels = jnp.arange(opening_tally)
        affinity_grades = jax.random.randint(rating_seed, (opening_tally,), 0, 1024) + extra_cluster[opening_labels // semi_cluster]
        affinity_grades = affinity_grades + 8192 * (opening_labels == slot_of[forward]) + 8192 * (opening_labels == slot_of[previous])
        affinity_grades = affinity_grades * opening_tally + opening_labels
        unused, chosen = lax.top_k(affinity_grades, cell_count)
        seating = jax.random.permutation(seat_key, TOK_DEV)
        cell_of = seating // CAP
        pair_ids = pair_table[chosen[cell_of]]
        flipped = jax.random.randint(flip_key, (TOK_DEV,), 0, 2)
        first_pick = jnp.where(flipped == 1, pair_ids[:, 1], pair_ids[:, 0])
        second_pick = jnp.where(flipped == 1, pair_ids[:, 0], pair_ids[:, 1])
        return jnp.stack([first_pick, second_pick], axis=1)
    table = jax.vmap(one_block)(jnp.arange(blocks))
    return table.reshape(TOKENS, 2)


def draw_routing(key, part):
    return route_table(key).astype(jnp.int32)


def block_levels(key, shape, pieces, low, top_value):
    loudness, own = 1.0, jax.random.fold_in(key, 6)
    for dim, blocks in pieces:
        steps = jnp.exp(jax.random.uniform(jax.random.fold_in(own, dim), (blocks,), jnp.float32, low / len(pieces), top_value / len(pieces)))
        loudness = loudness * jnp.repeat(steps, shape[dim] // blocks).reshape([-1 if axis == dim else 1 for axis in range(len(shape))])
    return loudness


def scatter_about(stream_key, extent, width, reach, pieces=(), kind=jnp.bfloat16):
    loudness = block_levels(stream_key, extent, pieces, -0.22, 0.18) if pieces else 1.0
    array = jax.random.normal(stream_key, extent, jnp.float32) * width * loudness
    return jnp.minimum(jnp.maximum(array, -reach), reach).astype(kind)


def setup_inputs(seed: int = 0) -> dict:
    key_of = jax.random.split(jax.random.key(seed), 8)
    return {
        "tokens": scatter_about(key_of[0], (TOKENS, D), 1.0, 6.0, ((0, 128), (1, 2))),
        "norm_gain": jnp.clip(1.0 + 0.18 * jax.random.normal(key_of[1], (D,), jnp.float32), 0.1, 1.9),
        "routing": draw_routing(jax.random.fold_in(key_of[7], 71), 0),
        "route_weight": jnp.clip(0.25 + 0.75 * jax.random.uniform(key_of[3], (TOKENS, TOP_K), jnp.float32) ** block_levels(key_of[3], (TOKENS, TOP_K), ((0, 128),), -0.2, 0.2), 0.25, 1.0),
        "w_gate": scatter_about(key_of[4], (EXPERTS, D, FFE), D ** -0.5, 0.1875, ((0, 128), (2, 2))),
        "w_up": scatter_about(key_of[5], (EXPERTS, D, FFE), D ** -0.5, 0.1875, ((0, 128), (2, 2))),
        "w_down": scatter_about(key_of[6], (EXPERTS, FFE, D), FFE ** -0.5, 0.25, ((0, 128), (2, 2))),
    }


epsilon = 1e-06

def reference(tokens, norm_gain, routing, route_weight, w_gate, w_up, w_down):
    row_span = 32
    float_rows = tokens.astype(jnp.float32)
    scale = lax.rsqrt(lax.optimization_barrier(jnp.mean(float_rows * float_rows, axis=1, keepdims=True)) + epsilon)
    normed = (float_rows * scale * norm_gain[None, :]).astype(jnp.bfloat16)
    count = TOKENS * TOP_K
    flat_expert = routing.reshape(-1).astype(jnp.int32)
    flat_token = (jnp.arange(count) // TOP_K).astype(jnp.int32)
    flat_weight = route_weight.reshape(-1)
    sorting = jnp.argsort(flat_expert, stable=True).astype(jnp.int32)
    sorted_expert = flat_expert[sorting]
    counts = jnp.zeros((EXPERTS,), jnp.int32).at[flat_expert].add(1)
    starts = (jnp.cumsum(counts) - counts).astype(jnp.int32)
    padded = ((counts + row_span - 1) // row_span * row_span).astype(jnp.int32)
    pad_end = jnp.cumsum(padded).astype(jnp.int32)
    pad_start = (pad_end - padded).astype(jnp.int32)
    target = (pad_start[sorted_expert] + jnp.arange(count).astype(jnp.int32) - starts[sorted_expert]).astype(jnp.int32)
    block_count = -(-count // row_span) + EXPERTS
    row_total = block_count * row_span
    buffer = jnp.zeros((row_total, D), jnp.bfloat16).at[target].set(normed[flat_token[sorting]])
    block_expert = jnp.searchsorted(pad_end, (jnp.arange(block_count) * row_span).astype(jnp.int32), side='right')
    block_expert = jnp.minimum(block_expert.astype(jnp.int32), EXPERTS - 1).astype(jnp.int32)

    def run_block(inputs):
        block_rows, expert = inputs
        gate_acc = jnp.dot(block_rows, w_gate[expert], preferred_element_type=jnp.float32)
        up_acc = jnp.dot(block_rows, w_up[expert], preferred_element_type=jnp.float32)
        hidden = (jax.nn.silu(gate_acc) * up_acc).astype(jnp.bfloat16)
        return jnp.dot(hidden, w_down[expert], preferred_element_type=jnp.float32).astype(jnp.bfloat16)
    result = lax.map(run_block, (buffer.reshape(block_count, row_span, D), block_expert)).reshape(row_total, D)
    picked = result[target].astype(jnp.float32) * flat_weight[sorting][:, None]
    combined = jax.ops.segment_sum(picked, flat_token[sorting], num_segments=TOKENS)
    return combined.astype(jnp.bfloat16)
```

```python
import functools

import jax
import jax.numpy as jnp
from jax import lax
from jax.experimental import pallas as pl
from jax.experimental.pallas import tpu as pltpu
from jax.sharding import Mesh, PartitionSpec as P

CAP = 8
EPS = 1e-06
INFO = 8
F32 = jnp.float32
BF16 = jnp.bfloat16


def iota(shape, dim):
    return lax.broadcasted_iota(jnp.int32, shape, dim)


def norm_kernel(own_ref, other_ref, gain_ref, route_ref, weight_ref, out_ref):
    rows, width = own_ref.shape
    own = own_ref[...].astype(F32)
    other = other_ref[...].astype(F32)
    total = jnp.sum(own * own, axis=1, keepdims=True) + jnp.sum(other * other, axis=1, keepdims=True)
    scale = lax.rsqrt(total / (2 * width) + EPS)
    out_ref[0:rows, :] = (own * scale * gain_ref[...]).astype(BF16)
    weight = weight_ref[...]
    high = weight.astype(BF16).astype(F32)
    middle = (weight - high).astype(BF16).astype(F32)
    low = weight - high - middle
    info = jnp.concatenate([route_ref[...].astype(F32), high, middle, low], axis=0)
    out_ref[rows:, :] = jnp.zeros((INFO, width), BF16)
    out_ref[rows:, 0:rows] = info.astype(BF16)


def dispatch_kernel(plane_ref, *refs):
    blocks, (out0_ref, out1_ref, slot_ref, weight_ref) = refs[:-4], refs[-4:]
    rows = blocks[0].shape[0] - INFO
    span = 2 * rows
    chips = out0_ref.shape[0]
    experts = 2 * chips
    first_expert = plane_ref[0] * experts
    earlier = (iota((span, span), 0) < iota((span, span), 1)) & (
        iota((span, span), 0) // rows == iota((span, span), 1) // rows
    )
    earlier = earlier.astype(F32).astype(BF16)
    lane = iota((1, span), 1)
    slots, weights = [], []
    for pair in range(len(blocks) // 2):
        a, b = blocks[2 * pair], blocks[2 * pair + 1]
        info = jnp.concatenate([a[rows:, 0:rows].astype(F32), b[rows:, 0:rows].astype(F32)], axis=1)
        tokens = jnp.concatenate([a[0:rows, :], b[0:rows, :]], axis=0)
        picks = [info[k : k + 1].astype(jnp.int32) - first_expert for k in range(2)]
        row = iota((experts, span), 0)
        named = (row == picks[0]) | (row == picks[1])
        ahead = jnp.dot(
            named.astype(F32).astype(BF16), earlier, preferred_element_type=F32
        )
        targets = []
        for k in range(2):
            rank = jnp.sum(jnp.where(row == picks[k], ahead, 0.0), axis=0, keepdims=True).astype(jnp.int32)
            inside = (picks[k] >= 0) & (picks[k] < experts)
            place = (picks[k] % 2) * (16 * chips) + (picks[k] // 2) * 16 + (lane // rows) * CAP + rank
            targets.append(jnp.where(inside, place, -1))
            slots.append(targets[k].astype(F32))
            weights.append(info[2 + k : 3 + k] + info[4 + k : 5 + k] + info[6 + k : 7 + k])
        for local, out_ref in enumerate((out0_ref, out1_ref)):
            slot = iota((16 * chips, span), 0) + local * 16 * chips
            chosen = ((slot == targets[0]) | (slot == targets[1])).astype(F32).astype(BF16)
            sent = jnp.dot(chosen, tokens, preferred_element_type=F32).astype(BF16)
            out_ref[:, 16 * pair : 16 * (pair + 1), :] = sent.reshape(chips, 16, -1)
    slot_ref[...] = jnp.concatenate(slots, axis=0)
    weight_ref[...] = jnp.concatenate(weights, axis=0)


def hidden_kernel(core_ref, own_ref, other_ref, gate_ref, up_ref, out_ref):
    core = core_ref[0]
    half = own_ref.shape[1]
    here = pl.ds(pl.multiple_of(core * half, half), half)
    there = pl.ds(pl.multiple_of((1 - core) * half, half), half)
    dot = functools.partial(jnp.dot, preferred_element_type=F32)
    gate = dot(own_ref[...], gate_ref[0, here, :]) + dot(other_ref[...], gate_ref[0, there, :])
    up = dot(own_ref[...], up_ref[0, here, :]) + dot(other_ref[...], up_ref[0, there, :])
    out_ref[...] = (gate / (1.0 + jnp.exp(-gate)) * up).astype(BF16)


def down_kernel(core_ref, own_ref, other_ref, down_ref, out_ref):
    core = core_ref[0]
    half = own_ref.shape[1]
    here = pl.ds(pl.multiple_of(core * half, half), half)
    there = pl.ds(pl.multiple_of((1 - core) * half, half), half)
    dot = functools.partial(jnp.dot, preferred_element_type=F32)
    out_ref[...] = (dot(own_ref[...], down_ref[0, here, :]) + dot(other_ref[...], down_ref[0, there, :])).astype(BF16)


def combine_kernel(plane_ref, back0_ref, back1_ref, slot_ref, weight_ref, out_ref):
    planes, rows, width = out_ref.shape
    chips = back0_ref.shape[0]
    span = 2 * rows
    plane = plane_ref[0]
    for pair in range(planes // 2):
        part = slice(16 * pair, 16 * (pair + 1))
        back = jnp.concatenate(
            [r[:, part, :].reshape(16 * chips, width) for r in (back0_ref, back1_ref)], axis=0
        )
        total = None
        for k in range(2):
            column = 2 * pair + k
            slot = slot_ref[:, column : column + 1].astype(jnp.int32)
            chosen = (iota((span, 32 * chips), 1) == slot).astype(F32).astype(BF16)
            picked = jnp.dot(chosen, back, preferred_element_type=F32)
            term = picked * weight_ref[:, column : column + 1]
            total = term if total is None else total + term
        total = total.astype(BF16)
        for side in range(2):
            out_ref[lax.rem(plane - (2 * pair + side) + planes, planes)] = total[side * rows : (side + 1) * rows]


def call(kernel, out_shape, args, flops, specs=None, **kw):
    moved = sum(a.size * a.dtype.itemsize for a in args)
    return pl.pallas_call(
        kernel,
        out_shape=out_shape,
        cost_estimate=pl.CostEstimate(flops=flops, bytes_accessed=moved, transcendentals=0),
        **kw,
    )(*args)


def local(tokens, norm_gain, routing, route_weight, w_gate, w_up, w_down):
    rows, half = tokens.shape
    planes = lax.axis_size("z")
    chips = lax.axis_size("y") * lax.axis_size("x")
    plane = lax.axis_index("z").astype(jnp.int32).reshape(1)
    core = lax.axis_index("tp").astype(jnp.int32).reshape(1)
    smem = pl.BlockSpec(memory_space=pltpu.SMEM)
    whole = pl.BlockSpec(memory_space=pltpu.VMEM)

    def swap(v):
        return lax.ppermute(v, "tp", [(0, 1), (1, 0)])

    other = swap(tokens)
    block = call(
        norm_kernel,
        jax.ShapeDtypeStruct((rows + INFO, half), BF16),
        (tokens, other, norm_gain.reshape(1, half), routing.T, route_weight.T),
        4 * rows * half,
    )

    right = [(i, (i + 1) % planes) for i in range(planes)]
    left = [(i, (i - 1) % planes) for i in range(planes)]
    blocks = [None] * planes
    blocks[0] = block
    up_going = down_going = block
    for step in range(1, planes // 2 + 1):
        up_going = lax.ppermute(up_going, "z", right)
        blocks[step] = up_going
        if planes - step > step:
            down_going = lax.ppermute(down_going, "z", left)
            blocks[planes - step] = down_going

    slots = planes * CAP
    shape = jax.ShapeDtypeStruct((chips, slots, half), BF16)
    small = jax.ShapeDtypeStruct((planes, 2 * rows), F32)
    sent0, sent1, place, weight = call(
        dispatch_kernel,
        (shape, shape, small, small),
        (plane, *blocks),
        4 * planes * chips * CAP * 2 * rows * half,
        in_specs=[smem] + [whole] * planes,
    )
    place, weight = place.T, weight.T
    back = []
    for index, sent in enumerate((sent0, sent1)):
        arrived = lax.all_to_all(sent, ("y", "x"), split_axis=0, concat_axis=0, tiled=True)
        arrived = arrived.reshape(chips * slots, half)
        total = arrived.shape[0]
        hidden_half = w_gate.shape[2]
        pick = lambda i: (index, 0, 0)
        hidden = call(
            hidden_kernel,
            jax.ShapeDtypeStruct((total, hidden_half), BF16),
            (core, arrived, swap(arrived), w_gate, w_up),
            8 * total * half * hidden_half,
            grid=(4,),
            in_specs=[
                smem,
                pl.BlockSpec((total // 4, half), lambda i: (i, 0)),
                pl.BlockSpec((total // 4, half), lambda i: (i, 0)),
                pl.BlockSpec((1, 2 * half, hidden_half), lambda i, index=index: (index, 0, 0)),
                pl.BlockSpec((1, 2 * half, hidden_half), lambda i, index=index: (index, 0, 0)),
            ],
            out_specs=pl.BlockSpec((total // 4, hidden_half), lambda i: (i, 0)),
        )
        result = call(
            down_kernel,
            jax.ShapeDtypeStruct((total, half), BF16),
            (core, hidden, swap(hidden), w_down),
            4 * total * half * hidden_half,
            grid=(4,),
            in_specs=[
                smem,
                pl.BlockSpec((total // 4, hidden_half), lambda i: (i, 0)),
                pl.BlockSpec((total // 4, hidden_half), lambda i: (i, 0)),
                pl.BlockSpec((1, 2 * hidden_half, half), lambda i, index=index: (index, 0, 0)),
            ],
            out_specs=pl.BlockSpec((total // 4, half), lambda i: (i, 0)),
        )
        back.append(
            lax.all_to_all(
                result.reshape(chips, slots, half), ("y", "x"), split_axis=0, concat_axis=0, tiled=True
            )
        )
    mixed = call(
        combine_kernel,
        jax.ShapeDtypeStruct((planes, rows, half), BF16),
        (plane, *back, place, weight),
        8 * planes * rows * 2 * chips * 16 * half,
        in_specs=[smem] + [whole] * 4,
    )
    home = lax.all_to_all(mixed, "z", split_axis=0, concat_axis=0, tiled=True)
    return jnp.sum(home.astype(F32), axis=0).astype(BF16)


def solution(mesh):
    mesh = Mesh(mesh.devices.reshape(8, 4, 4, 2), ("z", "y", "x", "tp"))
    ep = ("z", "y", "x")
    in_specs = (
        P(ep, "tp"),
        P("tp"),
        P(ep, None),
        P(ep, None),
        P(ep, None, "tp"),
        P(ep, None, "tp"),
        P(ep, None, "tp"),
    )
    return jax.shard_map(local, mesh=mesh, in_specs=in_specs, out_specs=P(ep, "tp"), check_vma=False)
```

```python
import functools

import jax
import jax.numpy as jnp
from jax import lax
from jax.experimental import pallas as pl
from jax.experimental.pallas import tpu as pltpu
from jax.sharding import PartitionSpec as P

CAP = 8
EPS = 1e-06
F32 = jnp.float32
BF16 = jnp.bfloat16
dot = functools.partial(jnp.dot, preferred_element_type=F32)


def iota(shape, dim):
    return lax.broadcasted_iota(jnp.int32, shape, dim)


def one_hot(mask):
    return mask.astype(F32).astype(BF16)


def dispatch_kernel(own_ref, other_ref, gain_ref, route_ref, out_ref, slot_ref):
    rows, half = own_ref.shape
    own = own_ref[...].astype(F32)
    other = other_ref[...].astype(F32)
    total = jnp.sum(own * own, axis=1, keepdims=True) + jnp.sum(other * other, axis=1, keepdims=True)
    scale = lax.rsqrt(total / (2 * half) + EPS)
    normed = (own * scale * gain_ref[...]).astype(BF16)

    peers, block, _ = out_ref.shape
    experts = peers * block // CAP
    expert = iota((experts, rows), 0)
    first, second = route_ref[0:1, :], route_ref[1:2, :]
    named = (expert == first) | (expert == second)
    earlier = one_hot(iota((rows, rows), 0) < iota((rows, rows), 1))
    ahead = dot(one_hot(named), earlier)
    slots = []
    for pick in (first, second):
        rank = jnp.sum(jnp.where(expert == pick, ahead, 0.0), axis=0, keepdims=True)
        slots.append(pick * CAP + rank.astype(jnp.int32))
    chunk = 256
    for at in range(0, peers * block, chunk):
        slot = iota((chunk, rows), 0) + at
        sent = dot(one_hot((slot == slots[0]) | (slot == slots[1])), normed).astype(BF16)
        out_ref[at // block : (at + chunk) // block] = sent.reshape(chunk // block, block, half)
    slot_ref[...] = jnp.concatenate(slots, axis=0)


def hidden_kernel(core_ref, own_ref, other_ref, gate_ref, up_ref, out_ref):
    core = core_ref[0]
    peers, block, half = own_ref.shape
    here = pl.ds(pl.multiple_of(core * half, half), half)
    there = pl.ds(pl.multiple_of((1 - core) * half, half), half)
    step = 256 // CAP
    for expert in range(block // CAP):
        for at in range(0, peers, step):
            part = (slice(at, at + step), slice(expert * CAP, (expert + 1) * CAP))
            own = own_ref[part].reshape(step * CAP, half)
            other = other_ref[part].reshape(step * CAP, half)
            gate = dot(own, gate_ref[expert, here, :]) + dot(other, gate_ref[expert, there, :])
            up = dot(own, up_ref[expert, here, :]) + dot(other, up_ref[expert, there, :])
            out_ref[expert, at * CAP : (at + step) * CAP] = (gate / (1.0 + jnp.exp(-gate)) * up).astype(BF16)


def down_kernel(core_ref, own_ref, other_ref, down_ref, out_ref):
    core = core_ref[0]
    experts, total, quarter = own_ref.shape
    here = pl.ds(pl.multiple_of(core * quarter, quarter), quarter)
    there = pl.ds(pl.multiple_of((1 - core) * quarter, quarter), quarter)
    step = 256
    for expert in range(experts):
        for at in range(0, total, step):
            part = slice(at, at + step)
            rows = dot(own_ref[expert, part], down_ref[expert, here, :]) + dot(
                other_ref[expert, part], down_ref[expert, there, :]
            )
            out_ref[at // CAP : (at + step) // CAP, expert * CAP : (expert + 1) * CAP] = (
                rows.astype(BF16).reshape(step // CAP, CAP, -1)
            )


def combine_kernel(back_ref, slot_ref, weight_ref, out_ref):
    peers, block, half = back_ref.shape
    rows = out_ref.shape[0]
    chunk = 256
    picked = [None, None]
    for at in range(0, peers * block, chunk):
        back = back_ref[at // block : (at + chunk) // block].reshape(chunk, half)
        place = iota((rows, chunk), 1) + at
        for k in range(2):
            term = dot(one_hot(place == slot_ref[:, k : k + 1]), back)
            picked[k] = term if picked[k] is None else picked[k] + term
    out_ref[...] = (picked[0] * weight_ref[:, 0:1] + picked[1] * weight_ref[:, 1:2]).astype(BF16)


def call(kernel, out_shape, args, flops, grant, scalars=0):
    moved = sum(a.size * a.dtype.itemsize for a in args)
    smem = pl.BlockSpec(memory_space=pltpu.SMEM)
    whole = pl.BlockSpec(memory_space=pltpu.VMEM)
    return pl.pallas_call(
        kernel,
        out_shape=out_shape,
        in_specs=[smem] * scalars + [whole] * (len(args) - scalars),
        cost_estimate=pl.CostEstimate(flops=flops, bytes_accessed=moved, transcendentals=0),
        compiler_params=pltpu.CompilerParams(vmem_limit_bytes=grant << 20),
    )(*args)


def local(tokens, norm_gain, routing, route_weight, w_gate, w_up, w_down):
    rows, half = tokens.shape
    peers = lax.axis_size("ep")
    experts, _, hidden_half = w_gate.shape
    block = experts * CAP
    core = lax.axis_index("tp").astype(jnp.int32).reshape(1)

    def swap(v):
        return lax.ppermute(v, "tp", [(0, 1), (1, 0)])

    def exchange(v):
        return lax.all_to_all(v, "ep", split_axis=0, concat_axis=0, tiled=True)

    buffer = jax.ShapeDtypeStruct((peers, block, half), BF16)
    sent, slots = call(
        dispatch_kernel,
        (buffer, jax.ShapeDtypeStruct((2, rows), jnp.int32)),
        (tokens, swap(tokens), norm_gain.reshape(1, half), routing.T),
        2 * peers * block * rows * half,
        12,
    )
    arrived = exchange(sent)
    hidden = call(
        hidden_kernel,
        jax.ShapeDtypeStruct((experts, peers * CAP, hidden_half), BF16),
        (core, arrived, swap(arrived), w_gate, w_up),
        8 * peers * block * half * hidden_half,
        20,
        1,
    )
    result = call(
        down_kernel, buffer, (core, hidden, swap(hidden), w_down), 4 * peers * block * hidden_half * half, 16, 1
    )
    back = exchange(result)
    return call(
        combine_kernel,
        jax.ShapeDtypeStruct((rows, half), BF16),
        (back, slots.T, route_weight),
        4 * peers * block * rows * half,
        12,
    )


def solution(mesh):
    in_specs = (
        P("ep", "tp"),
        P("tp"),
        P("ep", None),
        P("ep", None),
        P("ep", None, "tp"),
        P("ep", None, "tp"),
        P("ep", None, "tp"),
    )
    return jax.shard_map(local, mesh=mesh, in_specs=in_specs, out_specs=P("ep", "tp"), check_vma=False)
```

```python
import functools

import jax
import jax.numpy as jnp
from jax import lax
from jax.experimental import pallas as pl
from jax.experimental.pallas import tpu as pltpu
from jax.sharding import Mesh, PartitionSpec as P

CAP = 8
EPS = 1e-06
INFO = 8
F32 = jnp.float32
BF16 = jnp.bfloat16
dot = functools.partial(jnp.dot, preferred_element_type=F32)


def iota(shape, dim):
    return lax.broadcasted_iota(jnp.int32, shape, dim)


def one_hot(mask):
    return mask.astype(F32).astype(BF16)


def norm_kernel(own_ref, other_ref, gain_ref, route_ref, weight_ref, out_ref):
    rows, half = own_ref.shape
    own = own_ref[...].astype(F32)
    other = other_ref[...].astype(F32)
    total = jnp.sum(own * own, axis=1, keepdims=True) + jnp.sum(other * other, axis=1, keepdims=True)
    scale = lax.rsqrt(total / (2 * half) + EPS)
    out_ref[0:rows, :] = (own * scale * gain_ref[...]).astype(BF16)
    weight = weight_ref[...]
    high = weight.astype(BF16).astype(F32)
    middle = (weight - high).astype(BF16).astype(F32)
    low = weight - high - middle
    info = jnp.concatenate([route_ref[...].astype(F32), high, middle, low], axis=0)
    out_ref[rows:, :] = jnp.zeros((INFO, half), BF16)
    out_ref[rows:, 0:rows] = info.astype(BF16)


def dispatch_kernel(column_ref, *refs):
    blocks, (out_ref, table_ref) = refs[:-2], refs[-2:]
    rows = blocks[0].shape[0] - INFO
    span = 2 * rows
    peers, block, half = out_ref.shape
    experts = 2 * peers
    first_expert = column_ref[0] * experts
    earlier = one_hot(
        (iota((span, span), 0) < iota((span, span), 1))
        & (iota((span, span), 0) // rows == iota((span, span), 1) // rows)
    )
    side = iota((1, span), 1) // rows
    expert = iota((experts, span), 0)
    slots, weights = [], []
    for pair in range(len(blocks) // 2):
        a, b = blocks[2 * pair], blocks[2 * pair + 1]
        info = jnp.concatenate([a[rows:, 0:rows].astype(F32), b[rows:, 0:rows].astype(F32)], axis=1)
        tokens = jnp.concatenate([a[0:rows, :], b[0:rows, :]], axis=0)
        picks = [info[k : k + 1].astype(jnp.int32) - first_expert for k in range(2)]
        ahead = dot(one_hot((expert == picks[0]) | (expert == picks[1])), earlier)
        places = []
        for k in range(2):
            rank = jnp.sum(jnp.where(expert == picks[k], ahead, 0.0), axis=0, keepdims=True)
            inside = (picks[k] >= 0) & (picks[k] < experts)
            place = (picks[k] % 2) * (16 * peers) + (picks[k] // 2) * 16 + side * CAP + rank.astype(jnp.int32)
            places.append(jnp.where(inside, place, -1))
            slots.append(places[k].astype(F32))
            weights.append(info[2 + k : 3 + k] + info[4 + k : 5 + k] + info[6 + k : 7 + k])
        for local in range(2):
            at = local * (block // 2) + 16 * pair
            place = iota((16 * peers, span), 0) + local * 16 * peers
            sent = dot(one_hot((place == places[0]) | (place == places[1])), tokens)
            out_ref[:, at : at + 16, :] = sent.astype(BF16).reshape(peers, 16, half)
    table_ref[...] = jnp.concatenate(slots + weights, axis=0).T


def halves(core_ref, half):
    core = core_ref[0]
    here = pl.ds(pl.multiple_of(core * half, half), half)
    there = pl.ds(pl.multiple_of((1 - core) * half, half), half)
    return here, there


def half_kernel(core_ref, own_ref, gate_ref, up_ref, out_ref):
    peers, block, half = own_ref.shape
    width = gate_ref.shape[2]
    here, _ = halves(core_ref, half)
    part = block // 2
    step = 256 // part
    for expert in range(2):
        for at in range(0, peers, step):
            own = own_ref[at : at + step, expert * part : (expert + 1) * part].reshape(256, half)
            rows = slice(at * part, (at + step) * part)
            out_ref[expert, rows, 0:width] = dot(own, gate_ref[expert, here, :])
            out_ref[expert, rows, width:] = dot(own, up_ref[expert, here, :])


def hidden_kernel(core_ref, half_ref, other_ref, gate_ref, up_ref, out_ref):
    peers, block, half = other_ref.shape
    width = gate_ref.shape[2]
    _, there = halves(core_ref, half)
    part = block // 2
    step = 256 // part
    for expert in range(2):
        for at in range(0, peers, step):
            other = other_ref[at : at + step, expert * part : (expert + 1) * part].reshape(256, half)
            rows = slice(at * part, (at + step) * part)
            gate = half_ref[expert, rows, 0:width] + dot(other, gate_ref[expert, there, :])
            up = half_ref[expert, rows, width:] + dot(other, up_ref[expert, there, :])
            out_ref[expert, rows] = (gate / (1.0 + jnp.exp(-gate)) * up).astype(BF16)


def down_kernel(core_ref, own_ref, other_ref, down_ref, out_ref):
    experts, total, quarter = own_ref.shape
    here, there = halves(core_ref, quarter)
    peers, block, half = out_ref.shape
    part = block // 2
    step = 256 // part
    for expert in range(experts):
        for at in range(0, peers, step):
            rows = slice(at * part, (at + step) * part)
            result = dot(own_ref[expert, rows], down_ref[expert, here, :]) + dot(
                other_ref[expert, rows], down_ref[expert, there, :]
            )
            out_ref[at : at + step, expert * part : (expert + 1) * part] = result.astype(BF16).reshape(
                step, part, half
            )


def combine_kernel(column_ref, back_ref, table_ref, out_ref):
    columns, rows, half = out_ref.shape
    peers, block, _ = back_ref.shape
    span = 2 * rows
    for pair in range(columns // 2):
        picked = [None, None]
        for local in range(2):
            at = local * (block // 2) + 16 * pair
            back = back_ref[:, at : at + 16, :].reshape(16 * peers, half)
            place = iota((span, 16 * peers), 1) + local * 16 * peers
            for k in range(2):
                index = 2 * pair + k
                slot = table_ref[:, index : index + 1].astype(jnp.int32)
                term = dot(one_hot(place == slot), back)
                picked[k] = term if picked[k] is None else picked[k] + term
        index = columns + 2 * pair
        total = picked[0] * table_ref[:, index : index + 1] + picked[1] * table_ref[:, index + 1 : index + 2]
        total = total.astype(BF16)
        for side in range(2):
            to = lax.rem(column_ref[0] - (2 * pair + side) + columns, columns)
            out_ref[to] = total[side * rows : (side + 1) * rows]


def call(kernel, out_shape, args, flops, grant, scalars=0):
    moved = sum(a.size * a.dtype.itemsize for a in args)
    smem = pl.BlockSpec(memory_space=pltpu.SMEM)
    whole = pl.BlockSpec(memory_space=pltpu.VMEM)
    return pl.pallas_call(
        kernel,
        out_shape=out_shape,
        in_specs=[smem] * scalars + [whole] * (len(args) - scalars),
        cost_estimate=pl.CostEstimate(flops=flops, bytes_accessed=moved, transcendentals=0),
        compiler_params=pltpu.CompilerParams(vmem_limit_bytes=grant << 20),
    )(*args)


def local(tokens, norm_gain, routing, route_weight, w_gate, w_up, w_down):
    rows, half = tokens.shape
    columns = lax.axis_size("zh")
    plane = ("zl", "y", "x")
    peers = lax.axis_size(plane)
    experts, _, width = w_gate.shape
    block = experts * columns * CAP
    total = peers * block
    core = lax.axis_index("tp").astype(jnp.int32).reshape(1)
    column = lax.axis_index("zh").astype(jnp.int32).reshape(1)

    def swap(v):
        return lax.ppermute(v, "tp", [(0, 1), (1, 0)])

    def shift(v, by):
        return lax.ppermute(v, "zh", [(i, (i + by) % columns) for i in range(columns)])

    def exchange(v, axes):
        return lax.all_to_all(v, axes, split_axis=0, concat_axis=0, tiled=True)

    own = call(
        norm_kernel,
        jax.ShapeDtypeStruct((rows + INFO, half), BF16),
        (tokens, swap(tokens), norm_gain.reshape(1, half), routing.T, route_weight.T),
        4 * rows * half,
        4,
    )
    before, after = shift(own, 1), shift(own, -1)
    blocks = (own, before, shift(before, 1), after)

    buffer = jax.ShapeDtypeStruct((peers, block, half), BF16)
    sent, table = call(
        dispatch_kernel,
        (buffer, jax.ShapeDtypeStruct((2 * rows, 2 * columns), F32)),
        (column, *blocks),
        2 * total * 2 * rows * half,
        12,
        1,
    )
    arrived = exchange(sent, plane)
    other = swap(arrived)
    partial = call(
        half_kernel,
        jax.ShapeDtypeStruct((experts, total // experts, 2 * width), F32),
        (core, arrived, w_gate, w_up),
        4 * total * half * width,
        16,
        1,
    )
    hidden = call(
        hidden_kernel,
        jax.ShapeDtypeStruct((experts, total // experts, width), BF16),
        (core, partial, other, w_gate, w_up),
        4 * total * half * width,
        16,
        1,
    )
    result = call(down_kernel, buffer, (core, hidden, swap(hidden), w_down), 4 * total * width * half, 12, 1)
    back = exchange(result, plane)
    mixed = call(
        combine_kernel,
        jax.ShapeDtypeStruct((columns, rows, half), BF16),
        (column, back, table),
        4 * total * 2 * rows * half,
        12,
        1,
    )
    home = exchange(mixed, "zh")
    return jnp.sum(home.astype(F32), axis=0).astype(BF16)


def solution(mesh):
    mesh = Mesh(mesh.devices.reshape(4, 2, 4, 4, 2), ("zh", "zl", "y", "x", "tp"))
    ep = ("zh", "zl", "y", "x")
    in_specs = (
        P(ep, "tp"),
        P("tp"),
        P(ep, None),
        P(ep, None),
        P(ep, None, "tp"),
        P(ep, None, "tp"),
        P(ep, None, "tp"),
    )
    return jax.shard_map(local, mesh=mesh, in_specs=in_specs, out_specs=P(ep, "tp"), check_vma=False)
```

```python
import functools

import jax
import jax.numpy as jnp
from jax import lax
from jax.experimental import pallas as pl
from jax.experimental.pallas import tpu as pltpu
from jax.sharding import Mesh, PartitionSpec as P


CAP = 8
EPS = 1e-06
INFO = 8
F32 = jnp.float32
BF16 = jnp.bfloat16
dot = functools.partial(jnp.dot, preferred_element_type=F32)


def iota(shape, dim):
    return lax.broadcasted_iota(jnp.int32, shape, dim)


def one_hot(mask):
    return mask.astype(F32).astype(BF16)


def block_kernel(own_ref, gain_ref, route_ref, weight_ref, out_ref, total_ref, gain_out_ref):
    rows, half = own_ref.shape
    out_ref[0:rows, :] = own_ref[...]
    own = own_ref[...].astype(F32)
    total_ref[...] = jnp.broadcast_to(jnp.sum(own * own, axis=1, keepdims=True), total_ref.shape)
    gain_out_ref[...] = gain_ref[...]
    weight = weight_ref[...]
    high = weight.astype(BF16).astype(F32)
    middle = (weight - high).astype(BF16).astype(F32)
    low = weight - high - middle
    info = jnp.concatenate([route_ref[...].astype(F32), high, middle, low], axis=0)
    out_ref[rows:, :] = jnp.zeros((INFO, half), BF16)
    out_ref[rows:, 0:rows] = info.astype(BF16)


def norm_kernel(block_ref, total_ref, gain_ref, other_ref, out_ref):
    rows, half = other_ref.shape
    other = other_ref[...].astype(F32)
    total = total_ref[:, 0:1] + jnp.sum(other * other, axis=1, keepdims=True)
    scale = lax.rsqrt(total / (2 * half) + EPS)
    out_ref[0:rows, :] = (block_ref[0:rows, :].astype(F32) * scale * gain_ref[...]).astype(BF16)
    out_ref[rows:, :] = block_ref[rows:, :]


def dispatch_kernel(place_ref, *refs):
    blocks, (out_ref, table_ref) = refs[:-2], refs[-2:]
    rows = blocks[0].shape[0] - INFO
    span = 2 * rows
    peers, block, half = out_ref.shape
    experts = 2 * peers
    first_expert = place_ref[0] // 2 * experts
    earlier = one_hot(
        (iota((span, span), 0) < iota((span, span), 1))
        & (iota((span, span), 0) // rows == iota((span, span), 1) // rows)
    )
    side = iota((1, span), 1) // rows
    expert = iota((experts, span), 0)
    slots, weights = [], []
    for pair in range(len(blocks) // 2):
        a, b = blocks[2 * pair], blocks[2 * pair + 1]
        info = jnp.concatenate([a[rows:, 0:rows].astype(F32), b[rows:, 0:rows].astype(F32)], axis=1)
        tokens = jnp.concatenate([a[0:rows, :], b[0:rows, :]], axis=0)
        picks = [info[k : k + 1].astype(jnp.int32) - first_expert for k in range(2)]
        ahead = dot(one_hot((expert == picks[0]) | (expert == picks[1])), earlier)
        places = []
        for k in range(2):
            rank = jnp.sum(jnp.where(expert == picks[k], ahead, 0.0), axis=0, keepdims=True)
            inside = (picks[k] >= 0) & (picks[k] < experts)
            place = (picks[k] % 2) * (16 * peers) + (picks[k] // 2) * 16 + side * CAP + rank.astype(jnp.int32)
            places.append(jnp.where(inside, place, -1))
            slots.append(places[k].astype(F32))
            weights.append(info[2 + k : 3 + k] + info[4 + k : 5 + k] + info[6 + k : 7 + k])
        for local in range(2):
            at = local * (block // 2) + 16 * pair
            place = iota((16 * peers, span), 0) + local * 16 * peers
            sent = dot(one_hot((place == places[0]) | (place == places[1])), tokens)
            out_ref[:, at : at + 16, :] = sent.astype(BF16).reshape(peers, 16, half)
    table_ref[...] = jnp.concatenate(slots + weights, axis=0).T


def expert_kernel(place_ref, rows_ref, gate_ref, up_ref, gate2_ref, up2_ref, down_ref, down2_ref, out_ref):
    core = place_ref[0] % 2
    chips, _, block, half = rows_ref.shape
    width = gate_ref.shape[2]
    sides = (core, 1 - core)
    spans = [pl.ds(pl.multiple_of(side * width, width), width) for side in sides]
    step = 256 // block
    for at in range(0, chips, step):
        low = rows_ref[at : at + step, 0].reshape(256, half)
        high = rows_ref[at : at + step, 1].reshape(256, half)

        def through(ref):
            return dot(low, ref[core, 0:half, :]) + dot(high, ref[core, half:, :])

        hidden = []
        for gate_half, up_half in ((gate_ref, up_ref), (gate2_ref, up2_ref)):
            gate = through(gate_half)
            hidden.append((gate / (1.0 + jnp.exp(-gate)) * through(up_half)).astype(BF16))
        for side, down in zip(sides, (down_ref, down2_ref)):
            result = dot(hidden[0], down[core, spans[0], :]) + dot(hidden[1], down[core, spans[1], :])
            out_ref[at : at + step, side] = result.astype(BF16).reshape(step, block, half)


def combine_kernel(place_ref, back_ref, table_ref, out_ref):
    columns, rows, half = out_ref.shape
    peers, block, _ = back_ref.shape
    span = 2 * rows
    for pair in range(columns // 2):
        picked = [None, None]
        for local in range(2):
            at = local * (block // 2) + 16 * pair
            back = back_ref[:, at : at + 16, :].reshape(16 * peers, half)
            place = iota((span, 16 * peers), 1) + local * 16 * peers
            for k in range(2):
                index = 2 * pair + k
                slot = table_ref[:, index : index + 1].astype(jnp.int32)
                term = dot(one_hot(place == slot), back)
                picked[k] = term if picked[k] is None else picked[k] + term
        index = columns + 2 * pair
        total = picked[0] * table_ref[:, index : index + 1] + picked[1] * table_ref[:, index + 1 : index + 2]
        total = total.astype(BF16)
        for side in range(2):
            to = lax.rem(place_ref[0] // 2 - (2 * pair + side) + columns, columns)
            out_ref[to] = total[side * rows : (side + 1) * rows]


def call(kernel, out_shape, args, flops, grant, scalars=0, **kw):
    moved = sum(a.size * a.dtype.itemsize for a in args)
    smem = pl.BlockSpec(memory_space=pltpu.SMEM)
    whole = pl.BlockSpec(memory_space=pltpu.VMEM)
    kw.setdefault("in_specs", [smem] * scalars + [whole] * (len(args) - scalars))
    return pl.pallas_call(
        kernel,
        out_shape=out_shape,
        cost_estimate=pl.CostEstimate(flops=flops, bytes_accessed=moved, transcendentals=0),
        compiler_params=pltpu.CompilerParams(vmem_limit_bytes=grant << 20),
        **kw,
    )(*args)


def local(tokens, norm_gain, routing, route_weight, w_gate, w_up, w_down):
    rows, half = tokens.shape
    columns = lax.axis_size("zh")
    plane = ("zl", "y", "x", "tp")
    peers = lax.axis_size(plane) // 2
    experts, _, width = w_gate.shape
    block = experts * columns * CAP
    total = peers * block
    place = (lax.axis_index("zh") * 2 + lax.axis_index("tp")).astype(jnp.int32).reshape(1)

    def swap(v):
        return lax.ppermute(v, "tp", [(0, 1), (1, 0)])

    def shift(v, by):
        return lax.ppermute(v, "zh", [(i, (i + by) % columns) for i in range(columns)])

    def exchange(v, axes):
        return lax.all_to_all(v, axes, split_axis=0, concat_axis=0, tiled=True)

    other = swap(tokens)
    gate2, up2, down2 = swap(w_gate), swap(w_up), swap(w_down)
    own = call(
        block_kernel,
        (
            jax.ShapeDtypeStruct((rows + INFO, half), BF16),
            jax.ShapeDtypeStruct((rows, 128), F32),
            jax.ShapeDtypeStruct((1, half), F32),
        ),
        (tokens, norm_gain.reshape(1, half), routing.T, route_weight.T),
        rows * half,
        4,
    )
    own = call(norm_kernel, jax.ShapeDtypeStruct((rows + INFO, half), BF16), (*own, other), rows * half, 4)
    opposite, before, after = shift(own, 2), shift(own, 1), shift(own, -1)
    blocks = (own, before, opposite, after)

    sent, table = call(
        dispatch_kernel,
        (
            jax.ShapeDtypeStruct((peers, block, half), BF16),
            jax.ShapeDtypeStruct((2 * rows, 2 * columns), F32),
        ),
        (place, *blocks),
        2 * total * 2 * rows * half,
        12,
        1,
    )
    arrived = exchange(sent.reshape(2 * peers, block // 2, half), plane)
    result = call(
        expert_kernel,
        jax.ShapeDtypeStruct((peers, 2, block // 2, half), BF16),
        (place, arrived.reshape(peers, 2, block // 2, half), w_gate, w_up, gate2, up2, w_down, down2),
        total * half * width * 12,
        20,
        1,
    )
    back = exchange(result.reshape(2 * peers, block // 2, half), plane)
    mixed = call(
        combine_kernel,
        jax.ShapeDtypeStruct((columns, rows, half), BF16),
        (place, back.reshape(peers, block, half), table),
        4 * total * 2 * rows * half,
        12,
        1,
    )
    home = exchange(mixed, "zh")
    return jnp.sum(home.astype(F32), axis=0).astype(BF16)


def solution(mesh):
    mesh = Mesh(mesh.devices.reshape(4, 2, 4, 4, 2), ("zh", "zl", "y", "x", "tp"))
    ep = ("zh", "zl", "y", "x")
    in_specs = (
        P(ep, "tp"),
        P("tp"),
        P(ep, None),
        P(ep, None),
        P(ep, None, "tp"),
        P(ep, None, "tp"),
        P(ep, None, "tp"),
    )

    return jax.shard_map(local, mesh=mesh, in_specs=in_specs, out_specs=P(ep, "tp"), check_vma=False)
```

```python
import functools

import jax
import jax.numpy as jnp
from jax import lax
from jax.experimental import pallas as pl
from jax.experimental.pallas import tpu as pltpu
from jax.sharding import Mesh, PartitionSpec as P


CAP = 8
EPS = 1e-06
INFO = 8
F32 = jnp.float32
BF16 = jnp.bfloat16
dot = functools.partial(jnp.dot, preferred_element_type=F32)


def iota(shape, dim):
    return lax.broadcasted_iota(jnp.int32, shape, dim)


def one_hot(mask):
    return mask.astype(F32).astype(BF16)


def gather_kernel(own_ref, gain_ref, route_ref, weight_ref, out_ref):
    rows, half = own_ref.shape
    out_ref[0:rows, :] = own_ref[...].astype(F32)
    out_ref[rows : rows + 8, :] = jnp.broadcast_to(gain_ref[...], (8, half))
    weight = weight_ref[...]
    high = weight.astype(BF16).astype(F32)
    middle = (weight - high).astype(BF16).astype(F32)
    low = weight - high - middle
    out_ref[rows + 8 :, :] = jnp.zeros((INFO, half), F32)
    out_ref[rows + 8 :, 0:rows] = jnp.concatenate([route_ref[...].astype(F32), high, middle, low], axis=0)


def norm_kernel(held_ref, other_ref, out_ref):
    rows, half = other_ref.shape
    own = held_ref[0:rows, :]
    other = other_ref[...].astype(F32)
    total = jnp.sum(own * own, axis=1, keepdims=True) + jnp.sum(other * other, axis=1, keepdims=True)
    scale = lax.rsqrt(total / (2 * half) + EPS)
    out_ref[0:rows, :] = (own * scale * held_ref[rows : rows + 1, :]).astype(BF16)
    out_ref[rows:, :] = held_ref[rows + 8 :, :].astype(BF16)


def dispatch_kernel(place_ref, *refs):
    blocks, (out_ref, table_ref) = refs[:-2], refs[-2:]
    rows = blocks[0].shape[0] - INFO
    span = 2 * rows
    peers, block, half = out_ref.shape
    experts = 2 * peers
    first_expert = place_ref[0] // 2 * experts
    earlier = one_hot(
        (iota((span, span), 0) < iota((span, span), 1))
        & (iota((span, span), 0) // rows == iota((span, span), 1) // rows)
    )
    side = iota((1, span), 1) // rows
    expert = iota((experts, span), 0)
    slots, weights = [], []
    for pair in range(len(blocks) // 2):
        a, b = blocks[2 * pair], blocks[2 * pair + 1]
        info = jnp.concatenate([a[rows:, 0:rows].astype(F32), b[rows:, 0:rows].astype(F32)], axis=1)
        tokens = jnp.concatenate([a[0:rows, :], b[0:rows, :]], axis=0)
        picks = [info[k : k + 1].astype(jnp.int32) - first_expert for k in range(2)]
        ahead = dot(one_hot((expert == picks[0]) | (expert == picks[1])), earlier)
        places = []
        for k in range(2):
            rank = jnp.sum(jnp.where(expert == picks[k], ahead, 0.0), axis=0, keepdims=True)
            inside = (picks[k] >= 0) & (picks[k] < experts)
            place = (picks[k] % 2) * (16 * peers) + (picks[k] // 2) * 16 + side * CAP + rank.astype(jnp.int32)
            places.append(jnp.where(inside, place, -1))
            slots.append(places[k].astype(F32))
            weights.append(info[2 + k : 3 + k] + info[4 + k : 5 + k] + info[6 + k : 7 + k])
        for local in range(2):
            at = local * (block // 2) + 16 * pair
            place = iota((16 * peers, span), 0) + local * 16 * peers
            sent = dot(one_hot((place == places[0]) | (place == places[1])), tokens)
            out_ref[:, at : at + 16, :] = sent.astype(BF16).reshape(peers, 16, half)
    table_ref[...] = jnp.concatenate(slots + weights, axis=0).T


def hidden_part(rows_ref, at, gate_ref, up_ref, core):
    _, _, block, half = rows_ref.shape
    low, high = (rows_ref[at : at + 256 // block, side].reshape(256, half) for side in range(2))
    gate, up = (dot(low, ref[core, 0:half, :]) + dot(high, ref[core, half:, :]) for ref in (gate_ref, up_ref))
    return (gate / (1.0 + jnp.exp(-gate)) * up).astype(BF16)


def own_kernel(place_ref, rows_ref, gate_ref, up_ref, out_ref):
    chips, _, block, _ = rows_ref.shape
    for at in range(0, chips, 256 // block):
        out_ref[at * block : at * block + 256] = hidden_part(rows_ref, at, gate_ref, up_ref, place_ref[0] % 2)


def expert_kernel(place_ref, rows_ref, own_ref, gate2_ref, up2_ref, down_ref, down2_ref, out_ref):
    core = place_ref[0] % 2
    chips, _, block, half = rows_ref.shape
    width = own_ref.shape[1]
    sides = (core, 1 - core)
    spans = [pl.ds(pl.multiple_of(side * width, width), width) for side in sides]
    step = 256 // block
    for at in range(0, chips, step):
        own = own_ref[at * block : at * block + 256]
        other = hidden_part(rows_ref, at, gate2_ref, up2_ref, core)
        for side, down in zip(sides, (down_ref, down2_ref)):
            result = dot(own, down[core, spans[0], :]) + dot(other, down[core, spans[1], :])
            out_ref[at : at + step, side] = result.astype(BF16).reshape(step, block, half)


def combine_kernel(place_ref, back_ref, table_ref, out_ref):
    columns, rows, half = out_ref.shape
    peers, block, _ = back_ref.shape
    span = 2 * rows
    for pair in range(columns // 2):
        picked = [None, None]
        for local in range(2):
            at = local * (block // 2) + 16 * pair
            back = back_ref[:, at : at + 16, :].reshape(16 * peers, half)
            place = iota((span, 16 * peers), 1) + local * 16 * peers
            for k in range(2):
                index = 2 * pair + k
                slot = table_ref[:, index : index + 1].astype(jnp.int32)
                term = dot(one_hot(place == slot), back)
                picked[k] = term if picked[k] is None else picked[k] + term
        index = columns + 2 * pair
        total = picked[0] * table_ref[:, index : index + 1] + picked[1] * table_ref[:, index + 1 : index + 2]
        total = total.astype(BF16)
        for side in range(2):
            to = lax.rem(place_ref[0] // 2 - (2 * pair + side) + columns, columns)
            out_ref[to] = total[side * rows : (side + 1) * rows]


def call(kernel, out_shape, args, flops, grant, scalars=0, **kw):
    moved = sum(a.size * a.dtype.itemsize for a in args)
    smem = pl.BlockSpec(memory_space=pltpu.SMEM)
    whole = pl.BlockSpec(memory_space=pltpu.VMEM)
    kw.setdefault("in_specs", [smem] * scalars + [whole] * (len(args) - scalars))
    return pl.pallas_call(
        kernel,
        out_shape=out_shape,
        cost_estimate=pl.CostEstimate(flops=flops, bytes_accessed=moved, transcendentals=0),
        compiler_params=pltpu.CompilerParams(vmem_limit_bytes=grant << 20),
        **kw,
    )(*args)


def local(tokens, norm_gain, routing, route_weight, w_gate, w_up, w_down):
    rows, half = tokens.shape
    columns = lax.axis_size("zh")
    plane = ("zl", "y", "x", "tp")
    peers = lax.axis_size(plane) // 2
    experts, _, width = w_gate.shape
    block = experts * columns * CAP
    total = peers * block
    place = (lax.axis_index("zh") * 2 + lax.axis_index("tp")).astype(jnp.int32).reshape(1)

    def swap(v):
        return lax.ppermute(v, "tp", [(0, 1), (1, 0)])

    def shift(v, by):
        return lax.ppermute(v, "zh", [(i, (i + by) % columns) for i in range(columns)])

    def exchange(v, axes):
        return lax.all_to_all(v, axes, split_axis=0, concat_axis=0, tiled=True)

    other = swap(tokens)
    gate2, up2, down2 = swap(w_gate), swap(w_up), swap(w_down)
    held = call(
        gather_kernel,
        jax.ShapeDtypeStruct((rows + 8 + INFO, half), F32),
        (tokens, norm_gain.reshape(1, half), routing.T, route_weight.T),
        rows * half,
        60,
    )
    own = call(norm_kernel, jax.ShapeDtypeStruct((rows + INFO, half), BF16), (held, other), rows * half, 4)
    opposite, before, after = shift(own, 2), shift(own, 1), shift(own, -1)
    blocks = (own, before, opposite, after)

    sent, table = call(
        dispatch_kernel,
        (
            jax.ShapeDtypeStruct((peers, block, half), BF16),
            jax.ShapeDtypeStruct((2 * rows, 2 * columns), F32),
        ),
        (place, *blocks),
        2 * total * 2 * rows * half,
        12,
        1,
    )
    arrived = exchange(sent.reshape(2 * peers, block // 2, half), plane)
    arrived = arrived.reshape(peers, 2, block // 2, half)
    hidden = call(
        own_kernel,
        jax.ShapeDtypeStruct((total // 2, width), BF16),
        (place, arrived, w_gate, w_up),
        total * half * width * 4,
        12,
        1,
    )
    result = call(
        expert_kernel,
        jax.ShapeDtypeStruct((peers, 2, block // 2, half), BF16),
        (place, arrived, hidden, gate2, up2, w_down, down2),
        total * half * width * 8,
        16,
        1,
    )
    back = exchange(result.reshape(2 * peers, block // 2, half), plane)
    mixed = call(
        combine_kernel,
        jax.ShapeDtypeStruct((columns, rows, half), BF16),
        (place, back.reshape(peers, block, half), table),
        4 * total * 2 * rows * half,
        12,
        1,
    )
    home = exchange(mixed, "zh")
    return jnp.sum(home.astype(F32), axis=0).astype(BF16)


def solution(mesh):
    mesh = Mesh(mesh.devices.reshape(4, 2, 4, 4, 2), ("zh", "zl", "y", "x", "tp"))
    ep = ("zh", "zl", "y", "x")
    in_specs = (
        P(ep, "tp"),
        P("tp"),
        P(ep, None),
        P(ep, None),
        P(ep, None, "tp"),
        P(ep, None, "tp"),
        P(ep, None, "tp"),
    )

    return jax.shard_map(local, mesh=mesh, in_specs=in_specs, out_specs=P(ep, "tp"), check_vma=False)
```

```python
import functools

import jax
import jax.numpy as jnp
from jax import lax
from jax.experimental import pallas as pl
from jax.experimental.pallas import tpu as pltpu
from jax.sharding import Mesh, PartitionSpec as P


CAP = 8
EPS = 1e-06
INFO = 8
F32 = jnp.float32
BF16 = jnp.bfloat16
dot = functools.partial(jnp.dot, preferred_element_type=F32)


def iota(shape, dim):
    return lax.broadcasted_iota(jnp.int32, shape, dim)


def one_hot(mask):
    return mask.astype(F32).astype(BF16)


def gather_kernel(place_ref, own_ref, gain_ref, route_ref, weight_ref, out_ref):
    rows, half = own_ref.shape
    out_ref[0:rows, :] = own_ref[...].astype(F32)
    out_ref[rows : rows + 8, :] = jnp.broadcast_to(gain_ref[...], (8, half))
    weight = weight_ref[...]
    high = weight.astype(BF16).astype(F32)
    middle = (weight - high).astype(BF16).astype(F32)
    low = weight - high - middle
    out_ref[rows + 8 :, :] = jnp.zeros((INFO, half), F32)
    out_ref[rows + 8 :, 0:rows] = jnp.concatenate([route_ref[...].astype(F32), high, middle, low], axis=0)


def norm_kernel(held_ref, other_ref, out_ref):
    rows, half = other_ref.shape
    own = held_ref[0:rows, :]
    other = other_ref[...].astype(F32)
    total = jnp.sum(own * own, axis=1, keepdims=True) + jnp.sum(other * other, axis=1, keepdims=True)
    scale = lax.rsqrt(total / (2 * half) + EPS)
    normed = (own * scale * held_ref[rows : rows + 1, :]).astype(BF16)
    info = held_ref[rows + 8 :, :].astype(BF16)
    for peer in range(out_ref.shape[0]):
        out_ref[peer, 0:rows, :] = normed
        out_ref[peer, rows:, :] = info


def dispatch_kernel(place_ref, block_ref, out_ref, table_ref):
    columns, rows = block_ref.shape[0], block_ref.shape[1] - INFO
    span = 2 * rows
    peers, block, half = out_ref.shape
    experts = 2 * peers
    first_expert = place_ref[0] // 2 * experts
    earlier = one_hot(
        (iota((span, span), 0) < iota((span, span), 1))
        & (iota((span, span), 0) // rows == iota((span, span), 1) // rows)
    )
    side = iota((1, span), 1) // rows
    expert = iota((experts, span), 0)
    slots, weights = [], []
    for pair in range(columns // 2):
        a, b = block_ref.at[2 * pair], block_ref.at[2 * pair + 1]
        info = jnp.concatenate([a[rows:, 0:rows].astype(F32), b[rows:, 0:rows].astype(F32)], axis=1)
        tokens = jnp.concatenate([a[0:rows, :], b[0:rows, :]], axis=0)
        picks = [info[k : k + 1].astype(jnp.int32) - first_expert for k in range(2)]
        ahead = dot(one_hot((expert == picks[0]) | (expert == picks[1])), earlier)
        places = []
        for k in range(2):
            rank = jnp.sum(jnp.where(expert == picks[k], ahead, 0.0), axis=0, keepdims=True)
            inside = (picks[k] >= 0) & (picks[k] < experts)
            place = (picks[k] % 2) * (16 * peers) + (picks[k] // 2) * 16 + side * CAP + rank.astype(jnp.int32)
            places.append(jnp.where(inside, place, -1))
            slots.append(places[k].astype(F32))
            weights.append(info[2 + k : 3 + k] + info[4 + k : 5 + k] + info[6 + k : 7 + k])
        for local in range(2):
            at = local * (block // 2) + 16 * pair
            place = iota((16 * peers, span), 0) + local * 16 * peers
            sent = dot(one_hot((place == places[0]) | (place == places[1])), tokens)
            out_ref[:, at : at + 16, :] = sent.astype(BF16).reshape(peers, 16, half)
    table_ref[...] = jnp.concatenate(slots + weights, axis=0).T


def hidden_part(rows_ref, at, gate_ref, up_ref, core):
    _, _, block, half = rows_ref.shape
    low, high = (rows_ref[at : at + 256 // block, side].reshape(256, half) for side in range(2))
    gate, up = (dot(low, ref[core, 0:half, :]) + dot(high, ref[core, half:, :]) for ref in (gate_ref, up_ref))
    return (gate / (1.0 + jnp.exp(-gate)) * up).astype(BF16)


def own_kernel(place_ref, rows_ref, gate_ref, up_ref, out_ref):
    chips, _, block, _ = rows_ref.shape
    for at in range(0, chips, 256 // block):
        out_ref[at * block : at * block + 256] = hidden_part(rows_ref, at, gate_ref, up_ref, place_ref[0] % 2)


def expert_kernel(place_ref, rows_ref, own_ref, gate2_ref, up2_ref, down_ref, down2_ref, out_ref):
    core = place_ref[0] % 2
    chips, _, block, half = rows_ref.shape
    width = own_ref.shape[1]
    sides = (core, 1 - core)
    spans = [pl.ds(pl.multiple_of(side * width, width), width) for side in sides]
    step = 256 // block
    for at in range(0, chips, step):
        own = own_ref[at * block : at * block + 256]
        other = hidden_part(rows_ref, at, gate2_ref, up2_ref, core)
        for side, down in zip(sides, (down_ref, down2_ref)):
            result = dot(own, down[core, spans[0], :]) + dot(other, down[core, spans[1], :])
            out_ref[at : at + step, side] = result.astype(BF16).reshape(step, block, half)


def combine_kernel(back_ref, table_ref, out_ref):
    columns, rows, half = out_ref.shape
    peers, block, _ = back_ref.shape
    span = 2 * rows
    for pair in range(columns // 2):
        picked = [None, None]
        for local in range(2):
            at = local * (block // 2) + 16 * pair
            back = back_ref[:, at : at + 16, :].reshape(16 * peers, half)
            place = iota((span, 16 * peers), 1) + local * 16 * peers
            for k in range(2):
                index = 2 * pair + k
                slot = table_ref[:, index : index + 1].astype(jnp.int32)
                term = dot(one_hot(place == slot), back)
                picked[k] = term if picked[k] is None else picked[k] + term
        index = columns + 2 * pair
        total = picked[0] * table_ref[:, index : index + 1] + picked[1] * table_ref[:, index + 1 : index + 2]
        total = total.astype(BF16)
        for side in range(2):
            out_ref[2 * pair + side] = total[side * rows : (side + 1) * rows]


def call(kernel, out_shape, args, flops, grant, scalars=0, **kw):
    moved = sum(a.size * a.dtype.itemsize for a in args)
    smem = pl.BlockSpec(memory_space=pltpu.SMEM)
    whole = pl.BlockSpec(memory_space=pltpu.VMEM)
    kw.setdefault("in_specs", [smem] * scalars + [whole] * (len(args) - scalars))
    return pl.pallas_call(
        kernel,
        out_shape=out_shape,
        cost_estimate=pl.CostEstimate(flops=flops, bytes_accessed=moved, transcendentals=0),
        compiler_params=pltpu.CompilerParams(vmem_limit_bytes=grant << 20),
        **kw,
    )(*args)


def local(tokens, norm_gain, routing, route_weight, w_gate, w_up, w_down):
    rows, half = tokens.shape
    columns = lax.axis_size("zh")
    plane = ("zl", "y", "x", "tp")
    peers = lax.axis_size(plane) // 2
    experts, _, width = w_gate.shape
    block = experts * columns * CAP
    total = peers * block
    place = (lax.axis_index("zh") * 2 + lax.axis_index("tp")).astype(jnp.int32).reshape(1)

    def swap(v):
        return lax.ppermute(v, "tp", [(0, 1), (1, 0)])

    def exchange(v, axes):
        return lax.all_to_all(v, axes, split_axis=0, concat_axis=0, tiled=True)

    other = swap(tokens)
    gate2, up2, down2 = swap(w_gate), swap(w_up), swap(w_down)
    held = call(
        gather_kernel,
        jax.ShapeDtypeStruct((rows + 8 + INFO, half), F32),
        (place, tokens, norm_gain.reshape(1, half), routing.T, route_weight.T),
        rows * half,
        60,
        1,
    )
    own = call(norm_kernel, jax.ShapeDtypeStruct((columns, rows + INFO, half), BF16), (held, other), rows * half, 4)
    blocks = exchange(own, "zh")

    sent, table = call(
        dispatch_kernel,
        (
            jax.ShapeDtypeStruct((peers, block, half), BF16),
            jax.ShapeDtypeStruct((2 * rows, 2 * columns), F32),
        ),
        (place, blocks),
        2 * total * 2 * rows * half,
        12,
        1,
    )
    arrived = exchange(sent.reshape(2 * peers, block // 2, half), plane)
    arrived = arrived.reshape(peers, 2, block // 2, half)
    hidden = call(
        own_kernel,
        jax.ShapeDtypeStruct((total // 2, width), BF16),
        (place, arrived, w_gate, w_up),
        total * half * width * 4,
        12,
        1,
    )
    result = call(
        expert_kernel,
        jax.ShapeDtypeStruct((peers, 2, block // 2, half), BF16),
        (place, arrived, hidden, gate2, up2, w_down, down2),
        total * half * width * 8,
        16,
        1,
    )
    back = exchange(result.reshape(2 * peers, block // 2, half), plane)
    mixed = call(
        combine_kernel,
        jax.ShapeDtypeStruct((columns, rows, half), BF16),
        (back.reshape(peers, block, half), table),
        4 * total * 2 * rows * half,
        12,
    )
    home = exchange(mixed, "zh")
    return jnp.sum(home.astype(F32), axis=0).astype(BF16)


def solution(mesh):
    mesh = Mesh(mesh.devices.reshape(4, 2, 4, 4, 2), ("zh", "zl", "y", "x", "tp"))
    ep = ("zh", "zl", "y", "x")
    in_specs = (
        P(ep, "tp"),
        P("tp"),
        P(ep, None),
        P(ep, None),
        P(ep, None, "tp"),
        P(ep, None, "tp"),
        P(ep, None, "tp"),
    )

    return jax.shard_map(local, mesh=mesh, in_specs=in_specs, out_specs=P(ep, "tp"), check_vma=False)
```

```python
import functools

import jax
import jax.numpy as jnp
from jax import lax
from jax.experimental import pallas as pl
from jax.experimental.pallas import tpu as pltpu
from jax.sharding import Mesh, PartitionSpec as P


CAP = 8
EPS = 1e-06
INFO = 8
F32 = jnp.float32
BF16 = jnp.bfloat16
dot = functools.partial(jnp.dot, preferred_element_type=F32)


def iota(shape, dim):
    return lax.broadcasted_iota(jnp.int32, shape, dim)


def one_hot(mask):
    return mask.astype(F32).astype(BF16)


def gather_kernel(own_ref, gain_ref, route_ref, weight_ref, out_ref):
    rows, half = own_ref.shape
    out_ref[0:rows, :] = own_ref[...].astype(F32)
    out_ref[rows : rows + 8, :] = jnp.broadcast_to(gain_ref[...], (8, half))
    weight = weight_ref[...]
    high = weight.astype(BF16).astype(F32)
    middle = (weight - high).astype(BF16).astype(F32)
    low = weight - high - middle
    out_ref[rows + 8 :, :] = jnp.zeros((INFO, half), F32)
    out_ref[rows + 8 :, 0:rows] = jnp.concatenate([route_ref[...].astype(F32), high, middle, low], axis=0)


def norm_kernel(held_ref, other_ref, out_ref):
    rows, half = other_ref.shape
    own = held_ref[0:rows, :]
    other = other_ref[...].astype(F32)
    total = jnp.sum(own * own, axis=1, keepdims=True) + jnp.sum(other * other, axis=1, keepdims=True)
    scale = lax.rsqrt(total / (2 * half) + EPS)
    out_ref[0:rows, :] = (own * scale * held_ref[rows : rows + 1, :]).astype(BF16)
    out_ref[rows:, :] = held_ref[rows + 8 :, :].astype(BF16)


def dispatch_kernel(place_ref, *refs):
    blocks, (out_ref, table_ref) = refs[:-2], refs[-2:]
    rows = blocks[0].shape[0] - INFO
    span = 2 * rows
    peers, block, half = out_ref.shape
    experts = 2 * peers
    first_expert = place_ref[0] // 2 * experts
    earlier = one_hot(
        (iota((span, span), 0) < iota((span, span), 1))
        & (iota((span, span), 0) // rows == iota((span, span), 1) // rows)
    )
    side = iota((1, span), 1) // rows
    expert = iota((experts, span), 0)
    slots, weights = [], []
    for pair in range(len(blocks) // 2):
        a, b = blocks[2 * pair], blocks[2 * pair + 1]
        info = jnp.concatenate([a[rows:, 0:rows].astype(F32), b[rows:, 0:rows].astype(F32)], axis=1)
        tokens = jnp.concatenate([a[0:rows, :], b[0:rows, :]], axis=0)
        picks = [info[k : k + 1].astype(jnp.int32) - first_expert for k in range(2)]
        ahead = dot(one_hot((expert == picks[0]) | (expert == picks[1])), earlier)
        places = []
        for k in range(2):
            rank = jnp.sum(jnp.where(expert == picks[k], ahead, 0.0), axis=0, keepdims=True)
            inside = (picks[k] >= 0) & (picks[k] < experts)
            place = (picks[k] % 2) * (16 * peers) + (picks[k] // 2) * 16 + side * CAP + rank.astype(jnp.int32)
            places.append(jnp.where(inside, place, -1))
            slots.append(places[k].astype(F32))
            weights.append(info[2 + k : 3 + k] + info[4 + k : 5 + k] + info[6 + k : 7 + k])
        for local in range(2):
            at = local * (block // 2) + 16 * pair
            place = iota((16 * peers, span), 0) + local * 16 * peers
            sent = dot(one_hot((place == places[0]) | (place == places[1])), tokens)
            out_ref[:, at : at + 16, :] = sent.astype(BF16).reshape(peers, 16, half)
    table_ref[...] = jnp.concatenate(slots + weights, axis=0).T


def hidden_part(rows_ref, at, gate_ref, up_ref, core):
    _, _, block, half = rows_ref.shape
    low, high = (rows_ref[at : at + 256 // block, side].reshape(256, half) for side in range(2))
    gate, up = (dot(low, ref[core, 0:half, :]) + dot(high, ref[core, half:, :]) for ref in (gate_ref, up_ref))
    return (gate / (1.0 + jnp.exp(-gate)) * up).astype(BF16)


def own_kernel(place_ref, rows_ref, gate_ref, up_ref, out_ref):
    chips, _, block, _ = rows_ref.shape
    for at in range(0, chips, 256 // block):
        out_ref[at * block : at * block + 256] = hidden_part(rows_ref, at, gate_ref, up_ref, place_ref[0] % 2)


def expert_kernel(place_ref, rows_ref, own_ref, gate2_ref, up2_ref, down_ref, down2_ref, out_ref):
    core = place_ref[0] % 2
    chips, _, block, half = rows_ref.shape
    width = own_ref.shape[1]
    sides = (core, 1 - core)
    spans = [pl.ds(pl.multiple_of(side * width, width), width) for side in sides]
    step = 256 // block
    for at in range(0, chips, step):
        own = own_ref[at * block : at * block + 256]
        other = hidden_part(rows_ref, at, gate2_ref, up2_ref, core)
        for side, down in zip(sides, (down_ref, down2_ref)):
            result = dot(own, down[core, spans[0], :]) + dot(other, down[core, spans[1], :])
            out_ref[at : at + step, side] = result.astype(BF16).reshape(step, block, half)


def combine_kernel(back_ref, table_ref, *out_refs):
    columns, (rows, half) = len(out_refs), out_refs[0].shape
    peers, block, _ = back_ref.shape
    span = 2 * rows
    for pair in range(columns // 2):
        picked = [None, None]
        for local in range(2):
            at = local * (block // 2) + 16 * pair
            back = back_ref[:, at : at + 16, :].reshape(16 * peers, half)
            place = iota((span, 16 * peers), 1) + local * 16 * peers
            for k in range(2):
                index = 2 * pair + k
                slot = table_ref[:, index : index + 1].astype(jnp.int32)
                term = dot(one_hot(place == slot), back)
                picked[k] = term if picked[k] is None else picked[k] + term
        index = columns + 2 * pair
        total = picked[0] * table_ref[:, index : index + 1] + picked[1] * table_ref[:, index + 1 : index + 2]
        total = total.astype(BF16)
        for side in range(2):
            out_refs[2 * pair + side][...] = total[side * rows : (side + 1) * rows]


def call(kernel, out_shape, args, flops, grant, scalars=0, **kw):
    moved = sum(a.size * a.dtype.itemsize for a in args)
    smem = pl.BlockSpec(memory_space=pltpu.SMEM)
    whole = pl.BlockSpec(memory_space=pltpu.VMEM)
    kw.setdefault("in_specs", [smem] * scalars + [whole] * (len(args) - scalars))
    return pl.pallas_call(
        kernel,
        out_shape=out_shape,
        cost_estimate=pl.CostEstimate(flops=flops, bytes_accessed=moved, transcendentals=0),
        compiler_params=pltpu.CompilerParams(vmem_limit_bytes=grant << 20),
        **kw,
    )(*args)


def local(tokens, norm_gain, routing, route_weight, w_gate, w_up, w_down):
    rows, half = tokens.shape
    columns = lax.axis_size("zh")
    plane = ("zl", "y", "x", "tp")
    peers = lax.axis_size(plane) // 2
    experts, _, width = w_gate.shape
    block = experts * columns * CAP
    total = peers * block
    place = (lax.axis_index("zh") * 2 + lax.axis_index("tp")).astype(jnp.int32).reshape(1)

    def swap(v):
        return lax.ppermute(v, "tp", [(0, 1), (1, 0)])

    def shift(v, by):
        return lax.ppermute(v, "zh", [(i, (i + by) % columns) for i in range(columns)])

    def exchange(v, axes):
        return lax.all_to_all(v, axes, split_axis=0, concat_axis=0, tiled=True)

    other = swap(tokens)
    gate2, up2, down2 = swap(w_gate), swap(w_up), swap(w_down)
    held = call(
        gather_kernel,
        jax.ShapeDtypeStruct((rows + 8 + INFO, half), F32),
        (tokens, norm_gain.reshape(1, half), routing.T, route_weight.T),
        rows * half,
        60,
    )
    own = call(norm_kernel, jax.ShapeDtypeStruct((rows + INFO, half), BF16), (held, other), rows * half, 4)
    opposite, before, after = shift(own, 2), shift(own, 1), shift(own, -1)
    blocks = (own, before, opposite, after)

    sent, table = call(
        dispatch_kernel,
        (
            jax.ShapeDtypeStruct((peers, block, half), BF16),
            jax.ShapeDtypeStruct((2 * rows, 2 * columns), F32),
        ),
        (place, *blocks),
        2 * total * 2 * rows * half,
        12,
        1,
    )
    arrived = exchange(sent.reshape(2 * peers, block // 2, half), plane)
    arrived = arrived.reshape(peers, 2, block // 2, half)
    hidden = call(
        own_kernel,
        jax.ShapeDtypeStruct((total // 2, width), BF16),
        (place, arrived, w_gate, w_up),
        total * half * width * 4,
        12,
        1,
    )
    result = call(
        expert_kernel,
        jax.ShapeDtypeStruct((peers, 2, block // 2, half), BF16),
        (place, arrived, hidden, gate2, up2, w_down, down2),
        total * half * width * 8,
        16,
        1,
    )
    back = exchange(result.reshape(2 * peers, block // 2, half), plane)
    mixed = call(
        combine_kernel,
        (jax.ShapeDtypeStruct((rows, half), BF16),) * columns,
        (back.reshape(peers, block, half), table),
        4 * total * 2 * rows * half,
        12,
    )
    home = [shift(mixed[by], -by) for by in (2, 1, 3)]
    return sum((part.astype(F32) for part in home), mixed[0].astype(F32)).astype(BF16)


def solution(mesh):
    mesh = Mesh(mesh.devices.reshape(4, 2, 4, 4, 2), ("zh", "zl", "y", "x", "tp"))
    ep = ("zh", "zl", "y", "x")
    in_specs = (
        P(ep, "tp"),
        P("tp"),
        P(ep, None),
        P(ep, None),
        P(ep, None, "tp"),
        P(ep, None, "tp"),
        P(ep, None, "tp"),
    )

    return jax.shard_map(local, mesh=mesh, in_specs=in_specs, out_specs=P(ep, "tp"), check_vma=False)
```

```python
import functools

import jax
import jax.numpy as jnp
from jax import lax
from jax.experimental import pallas as pl
from jax.experimental.pallas import tpu as pltpu
from jax.sharding import Mesh, PartitionSpec as P


CAP = 8
EPS = 1e-06
INFO = 8
F32 = jnp.float32
BF16 = jnp.bfloat16
dot = functools.partial(jnp.dot, preferred_element_type=F32)


def iota(shape, dim):
    return lax.broadcasted_iota(jnp.int32, shape, dim)


def one_hot(mask):
    return mask.astype(F32).astype(BF16)


def parts(value):
    high = value.astype(BF16).astype(F32)
    middle = (value - high).astype(BF16).astype(F32)
    return [high, middle, value - high - middle]


def gather_kernel(own_ref, gain_ref, route_ref, weight_ref, out_ref):
    rows, half = own_ref.shape
    out_ref[0:rows, :] = own_ref[...]
    pad = jnp.zeros((5, half), F32)
    out_ref[rows:, :] = jnp.concatenate(
        [jnp.zeros((INFO, half), F32), *parts(gain_ref[...]), pad], axis=0
    ).astype(BF16)
    info = jnp.concatenate([route_ref[...].astype(F32), *parts(weight_ref[...])], axis=0)
    out_ref[rows : rows + INFO, 0:rows] = info.astype(BF16)


def norm_kernel(held_ref, other_ref, out_ref):
    rows, half = other_ref.shape
    own = held_ref[0:rows, :].astype(F32)
    other = other_ref[...].astype(F32)
    total = jnp.sum(own * own, axis=1, keepdims=True) + jnp.sum(other * other, axis=1, keepdims=True)
    scale = lax.rsqrt(total / (2 * half) + EPS)
    tail = held_ref[rows:, :]
    gain = tail[INFO:, :].astype(F32)
    gain = gain[0:1] + gain[1:2] + gain[2:3]
    out_ref[0:rows, :] = (own * scale * gain).astype(BF16)
    out_ref[rows:, :] = tail[0:INFO, :]


def dispatch_kernel(place_ref, own_ref, before_ref, opposite_ref, after_ref, out_ref, table0_ref, table1_ref):
    place_pair(0, place_ref, own_ref, before_ref, out_ref, table0_ref)
    place_pair(1, place_ref, opposite_ref, after_ref, out_ref, table1_ref)


def place_pair(pair, place_ref, a_ref, b_ref, out_ref, table_ref):
    rows = a_ref.shape[0] - INFO
    span = 2 * rows
    peers, block, half = out_ref.shape
    experts = 2 * peers
    earlier = one_hot(
        (iota((span, span), 0) < iota((span, span), 1))
        & (iota((span, span), 0) // rows == iota((span, span), 1) // rows)
    )
    side = iota((1, span), 1) // rows
    expert = iota((experts, span), 0)
    info = jnp.concatenate([a_ref[rows:, 0:rows].astype(F32), b_ref[rows:, 0:rows].astype(F32)], axis=1)
    tokens = jnp.concatenate([a_ref[0:rows, :], b_ref[0:rows, :]], axis=0)
    picks = [info[k : k + 1].astype(jnp.int32) - place_ref[0] // 2 * experts for k in range(2)]
    ahead = dot(one_hot((expert == picks[0]) | (expert == picks[1])), earlier)
    slots, weights = [], []
    for k, pick in enumerate(picks):
        rank = jnp.sum(jnp.where(expert == pick, ahead, 0.0), axis=0, keepdims=True).astype(jnp.int32)
        slot = (pick % 2) * (16 * peers) + (pick // 2) * 16 + side * CAP + rank
        slots.append(jnp.where((pick >= 0) & (pick < experts), slot, -1))
        weights.append(info[2 + k : 3 + k] + info[4 + k : 5 + k] + info[6 + k : 7 + k])
    for local in range(2):
        at = local * (block // 2) + 16 * pair
        slot = iota((16 * peers, span), 0) + local * 16 * peers
        sent = dot(one_hot((slot == slots[0]) | (slot == slots[1])), tokens)
        out_ref[:, at : at + 16, :] = sent.astype(BF16).reshape(peers, 16, half)
    columns = [slot.astype(F32) for slot in slots] + weights
    table_ref[...] = jnp.concatenate(columns + columns, axis=0).T


def hidden_part(rows_ref, at, gate_ref, up_ref, core):
    _, _, block, half = rows_ref.shape
    low, high = (rows_ref[at : at + 256 // block, side].reshape(256, half) for side in range(2))
    gate, up = (dot(low, ref[core, 0:half, :]) + dot(high, ref[core, half:, :]) for ref in (gate_ref, up_ref))
    return (gate / (1.0 + jnp.exp(-gate)) * up).astype(BF16)


def own_kernel(place_ref, rows_ref, gate_ref, up_ref, out_ref):
    chips, _, block, _ = rows_ref.shape
    for at in range(0, chips, 256 // block):
        out_ref[at * block : at * block + 256] = hidden_part(rows_ref, at, gate_ref, up_ref, place_ref[0] % 2)


def expert_kernel(place_ref, rows_ref, own_ref, gate2_ref, up2_ref, down_ref, down2_ref, out_ref):
    core = place_ref[0] % 2
    chips, _, block, half = rows_ref.shape
    width = own_ref.shape[1]
    sides = (core, 1 - core)
    spans = [pl.ds(pl.multiple_of(side * width, width), width) for side in sides]
    step = 256 // block
    for at in range(0, chips, step):
        own = own_ref[at * block : at * block + 256]
        other = hidden_part(rows_ref, at, gate2_ref, up2_ref, core)
        for side, down in zip(sides, (down_ref, down2_ref)):
            result = dot(own, down[core, spans[0], :]) + dot(other, down[core, spans[1], :])
            out_ref[at : at + step, side] = result.astype(BF16).reshape(step, block, half)


def combine_kernel(pair, back_ref, table_ref, a_ref, b_ref):
    rows, half = a_ref.shape
    peers, block, _ = back_ref.shape
    picked = [None, None]
    for local in range(2):
        at = local * (block // 2) + 16 * pair
        back = back_ref[:, at : at + 16, :].reshape(16 * peers, half)
        place = iota((2 * rows, 16 * peers), 1) + local * 16 * peers
        for k in range(2):
            term = dot(one_hot(place == table_ref[:, k : k + 1].astype(jnp.int32)), back)
            picked[k] = term if picked[k] is None else picked[k] + term
    total = (picked[0] * table_ref[:, 2:3] + picked[1] * table_ref[:, 3:4]).astype(BF16)
    a_ref[...] = total[0:rows]
    b_ref[...] = total[rows:]


def call(kernel, out_shape, args, flops, grant, scalars=0, **kw):
    moved = sum(a.size * a.dtype.itemsize for a in args)
    smem = pl.BlockSpec(memory_space=pltpu.SMEM)
    whole = pl.BlockSpec(memory_space=pltpu.VMEM)
    kw.setdefault("in_specs", [smem] * scalars + [whole] * (len(args) - scalars))
    return pl.pallas_call(
        kernel,
        out_shape=out_shape,
        cost_estimate=pl.CostEstimate(flops=flops, bytes_accessed=moved, transcendentals=0),
        compiler_params=pltpu.CompilerParams(vmem_limit_bytes=grant << 20),
        **kw,
    )(*args)


def local(tokens, norm_gain, routing, route_weight, w_gate, w_up, w_down):
    rows, half = tokens.shape
    columns = lax.axis_size("zh")
    plane = ("zl", "y", "x", "tp")
    peers = lax.axis_size(plane) // 2
    experts, _, width = w_gate.shape
    block = experts * columns * CAP
    total = peers * block
    place = (lax.axis_index("zh") * 2 + lax.axis_index("tp")).astype(jnp.int32).reshape(1)

    def swap(v):
        return lax.ppermute(v, "tp", [(0, 1), (1, 0)])

    def shift(v, by):
        return lax.ppermute(v, "zh", [(i, (i + by) % columns) for i in range(columns)])

    def exchange(v, axes):
        return lax.all_to_all(v, axes, split_axis=0, concat_axis=0, tiled=True)

    other = swap(tokens)
    gate2, up2, down2 = swap(w_gate), swap(w_up), swap(w_down)
    held = call(
        gather_kernel,
        jax.ShapeDtypeStruct((rows + INFO + 8, half), BF16),
        (tokens, norm_gain.reshape(1, half), routing.T, route_weight.T),
        rows * half,
        60,
    )
    own = call(norm_kernel, jax.ShapeDtypeStruct((rows + INFO, half), BF16), (held, other), rows * half, 4)
    opposite = shift(own, 2)
    before, after = shift(own, 1), shift(own, -1)

    buffer = jax.ShapeDtypeStruct((peers, block, half), BF16)
    small = jax.ShapeDtypeStruct((2 * rows, 8), F32)
    flops = total * 2 * rows * half
    sent, table0, table1 = call(
        dispatch_kernel, (buffer, small, small), (place, own, before, opposite, after), 2 * flops, 12, 1
    )
    arrived = exchange(sent.reshape(2 * peers, block // 2, half), plane)
    arrived = arrived.reshape(peers, 2, block // 2, half)
    hidden = call(
        own_kernel,
        jax.ShapeDtypeStruct((total // 2, width), BF16),
        (place, arrived, w_gate, w_up),
        total * half * width * 4,
        12,
        1,
    )
    result = call(
        expert_kernel,
        jax.ShapeDtypeStruct((peers, 2, block // 2, half), BF16),
        (place, arrived, hidden, gate2, up2, w_down, down2),
        total * half * width * 8,
        16,
        1,
    )
    back = exchange(result.reshape(2 * peers, block // 2, half), plane)
    back = back.reshape(peers, block, half)
    pair = (jax.ShapeDtypeStruct((rows, half), BF16),) * 2
    opposite, after = call(functools.partial(combine_kernel, 1), pair, (back, table1), 2 * flops, 8)
    own, before = call(functools.partial(combine_kernel, 0), pair, (back, table0), 2 * flops, 8)
    home = [shift(opposite, -2)]
    home += [shift(after, 1), shift(before, -1)]
    return sum((part.astype(F32) for part in home), own.astype(F32)).astype(BF16)


def solution(mesh):
    mesh = Mesh(mesh.devices.reshape(4, 2, 4, 4, 2), ("zh", "zl", "y", "x", "tp"))
    ep = ("zh", "zl", "y", "x")
    in_specs = (
        P(ep, "tp"),
        P("tp"),
        P(ep, None),
        P(ep, None),
        P(ep, None, "tp"),
        P(ep, None, "tp"),
        P(ep, None, "tp"),
    )

    return jax.shard_map(local, mesh=mesh, in_specs=in_specs, out_specs=P(ep, "tp"), check_vma=False)
```

```python
import functools

import jax
import jax.numpy as jnp
from jax import lax
from jax.experimental import pallas as pl
from jax.experimental.pallas import tpu as pltpu
from jax.sharding import Mesh, PartitionSpec as P


CAP = 8
EPS = 1e-06
INFO = 8
F32 = jnp.float32
BF16 = jnp.bfloat16
dot = functools.partial(jnp.dot, preferred_element_type=F32)


def iota(shape, dim):
    return lax.broadcasted_iota(jnp.int32, shape, dim)


def one_hot(mask):
    return mask.astype(F32).astype(BF16)


def parts(value):
    high = value.astype(BF16).astype(F32)
    middle = (value - high).astype(BF16).astype(F32)
    return [high, middle, value - high - middle]


def gather_kernel(own_ref, gain_ref, route_ref, weight_ref, out_ref):
    rows, half = own_ref.shape
    out_ref[0:rows, :] = own_ref[...]
    pad = jnp.zeros((5, half), F32)
    out_ref[rows:, :] = jnp.concatenate(
        [jnp.zeros((INFO, half), F32), *parts(gain_ref[...]), pad], axis=0
    ).astype(BF16)
    info = jnp.concatenate([route_ref[...].astype(F32), *parts(weight_ref[...])], axis=0)
    out_ref[rows : rows + INFO, 0:rows] = info.astype(BF16)


def norm_kernel(held_ref, other_ref, out_ref):
    rows, half = other_ref.shape
    own = held_ref[0:rows, :].astype(F32)
    other = other_ref[...].astype(F32)
    total = jnp.sum(own * own, axis=1, keepdims=True) + jnp.sum(other * other, axis=1, keepdims=True)
    scale = lax.rsqrt(total / (2 * half) + EPS)
    tail = held_ref[rows:, :]
    gain = tail[INFO:, :].astype(F32)
    gain = gain[0:1] + gain[1:2] + gain[2:3]
    out_ref[0:rows, :] = (own * scale * gain).astype(BF16)
    out_ref[rows:, :] = tail[0:INFO, :]


def dispatch_kernel(place_ref, own_ref, before_ref, opposite_ref, after_ref, out_ref, table0_ref, table1_ref):
    place_pair(0, place_ref, own_ref, before_ref, out_ref, table0_ref)
    place_pair(1, place_ref, opposite_ref, after_ref, out_ref, table1_ref)


def place_pair(pair, place_ref, a_ref, b_ref, out_ref, table_ref):
    rows = a_ref.shape[0] - INFO
    span = 2 * rows
    peers, block, half = out_ref.shape
    experts = 2 * peers
    earlier = one_hot(
        (iota((span, span), 0) < iota((span, span), 1))
        & (iota((span, span), 0) // rows == iota((span, span), 1) // rows)
    )
    side = iota((1, span), 1) // rows
    expert = iota((experts, span), 0)
    info = jnp.concatenate([a_ref[rows:, 0:rows].astype(F32), b_ref[rows:, 0:rows].astype(F32)], axis=1)
    tokens = jnp.concatenate([a_ref[0:rows, :], b_ref[0:rows, :]], axis=0)
    picks = [info[k : k + 1].astype(jnp.int32) - place_ref[0] // 2 * experts for k in range(2)]
    ahead = dot(one_hot((expert == picks[0]) | (expert == picks[1])), earlier)
    slots, weights = [], []
    for k, pick in enumerate(picks):
        rank = jnp.sum(jnp.where(expert == pick, ahead, 0.0), axis=0, keepdims=True).astype(jnp.int32)
        slot = (pick % 2) * (16 * peers) + (pick // 2) * 16 + side * CAP + rank
        slots.append(jnp.where((pick >= 0) & (pick < experts), slot, -1))
        weights.append(info[2 + k : 3 + k] + info[4 + k : 5 + k] + info[6 + k : 7 + k])
    for local in range(2):
        at = local * (block // 2) + 16 * pair
        slot = iota((16 * peers, span), 0) + local * 16 * peers
        sent = dot(one_hot((slot == slots[0]) | (slot == slots[1])), tokens)
        out_ref[:, at : at + 16, :] = sent.astype(BF16).reshape(peers, 16, half)
    columns = [slot.astype(F32) for slot in slots] + weights
    table_ref[...] = jnp.concatenate(columns + columns, axis=0).T


STEP = 512


def hidden_part(rows_ref, at, gate_ref, up_ref, core):
    _, _, block, half = rows_ref.shape
    low, high = (rows_ref[at : at + STEP // block, side].reshape(STEP, half) for side in range(2))
    gate, up = (dot(low, ref[core, 0:half, :]) + dot(high, ref[core, half:, :]) for ref in (gate_ref, up_ref))
    return (gate / (1.0 + jnp.exp(-gate)) * up).astype(BF16)


def own_kernel(place_ref, rows_ref, gate_ref, up_ref, out_ref):
    chips, _, block, _ = rows_ref.shape
    for at in range(0, chips, STEP // block):
        out_ref[at * block : at * block + STEP] = hidden_part(rows_ref, at, gate_ref, up_ref, place_ref[0] % 2)


def expert_kernel(place_ref, rows_ref, own_ref, gate2_ref, up2_ref, down_ref, down2_ref, out_ref):
    core = place_ref[0] % 2
    chips, _, block, half = rows_ref.shape
    width = own_ref.shape[1]
    sides = (core, 1 - core)
    spans = [pl.ds(pl.multiple_of(side * width, width), width) for side in sides]
    step = STEP // block
    for at in range(0, chips, step):
        own = own_ref[at * block : at * block + STEP]
        other = hidden_part(rows_ref, at, gate2_ref, up2_ref, core)
        for side, down in zip(sides, (down_ref, down2_ref)):
            result = dot(own, down[core, spans[0], :]) + dot(other, down[core, spans[1], :])
            out_ref[at : at + step, side] = result.astype(BF16).reshape(step, block, half)


def combine_kernel(pair, back_ref, table_ref, a_ref, b_ref):
    rows, half = a_ref.shape
    peers, block, _ = back_ref.shape
    picked = [None, None]
    for local in range(2):
        at = local * (block // 2) + 16 * pair
        back = back_ref[:, at : at + 16, :].reshape(16 * peers, half)
        place = iota((2 * rows, 16 * peers), 1) + local * 16 * peers
        for k in range(2):
            term = dot(one_hot(place == table_ref[:, k : k + 1].astype(jnp.int32)), back)
            picked[k] = term if picked[k] is None else picked[k] + term
    total = (picked[0] * table_ref[:, 2:3] + picked[1] * table_ref[:, 3:4]).astype(BF16)
    a_ref[...] = total[0:rows]
    b_ref[...] = total[rows:]


def call(kernel, out_shape, args, flops, grant, scalars=0, **kw):
    moved = sum(a.size * a.dtype.itemsize for a in args)
    smem = pl.BlockSpec(memory_space=pltpu.SMEM)
    whole = pl.BlockSpec(memory_space=pltpu.VMEM)
    kw.setdefault("in_specs", [smem] * scalars + [whole] * (len(args) - scalars))
    return pl.pallas_call(
        kernel,
        out_shape=out_shape,
        cost_estimate=pl.CostEstimate(flops=flops, bytes_accessed=moved, transcendentals=0),
        compiler_params=pltpu.CompilerParams(vmem_limit_bytes=grant << 20),
        **kw,
    )(*args)


def local(tokens, norm_gain, routing, route_weight, w_gate, w_up, w_down):
    rows, half = tokens.shape
    columns = lax.axis_size("zh")
    plane = ("zl", "y", "x", "tp")
    peers = lax.axis_size(plane) // 2
    experts, _, width = w_gate.shape
    block = experts * columns * CAP
    total = peers * block
    place = (lax.axis_index("zh") * 2 + lax.axis_index("tp")).astype(jnp.int32).reshape(1)

    def swap(v):
        return lax.ppermute(v, "tp", [(0, 1), (1, 0)])

    def shift(v, by):
        return lax.ppermute(v, "zh", [(i, (i + by) % columns) for i in range(columns)])

    def exchange(v, axes):
        return lax.all_to_all(v, axes, split_axis=0, concat_axis=0, tiled=True)

    other = swap(tokens)
    gate2, up2, down2 = swap(w_gate), swap(w_up), swap(w_down)
    held = call(
        gather_kernel,
        jax.ShapeDtypeStruct((rows + INFO + 8, half), BF16),
        (tokens, norm_gain.reshape(1, half), routing.T, route_weight.T),
        rows * half,
        60,
    )
    own = call(norm_kernel, jax.ShapeDtypeStruct((rows + INFO, half), BF16), (held, other), rows * half, 4)
    opposite = shift(own, 2)
    before, after = shift(own, 1), shift(own, -1)

    buffer = jax.ShapeDtypeStruct((peers, block, half), BF16)
    small = jax.ShapeDtypeStruct((2 * rows, 8), F32)
    flops = total * 2 * rows * half
    sent, table0, table1 = call(
        dispatch_kernel, (buffer, small, small), (place, own, before, opposite, after), 2 * flops, 12, 1
    )
    arrived = exchange(sent.reshape(2 * peers, block // 2, half), plane)
    arrived = arrived.reshape(peers, 2, block // 2, half)
    hidden = call(
        own_kernel,
        jax.ShapeDtypeStruct((total // 2, width), BF16),
        (place, arrived, w_gate, w_up),
        total * half * width * 4,
        12,
        1,
    )
    result = call(
        expert_kernel,
        jax.ShapeDtypeStruct((peers, 2, block // 2, half), BF16),
        (place, arrived, hidden, gate2, up2, w_down, down2),
        total * half * width * 8,
        16,
        1,
    )
    back = exchange(result.reshape(2 * peers, block // 2, half), plane)
    back = back.reshape(peers, block, half)
    pair = (jax.ShapeDtypeStruct((rows, half), BF16),) * 2
    opposite, after = call(functools.partial(combine_kernel, 1), pair, (back, table1), 2 * flops, 8)
    own, before = call(functools.partial(combine_kernel, 0), pair, (back, table0), 2 * flops, 8)
    home = [shift(opposite, -2)]
    home += [shift(after, 1), shift(before, -1)]
    return sum((part.astype(F32) for part in home), own.astype(F32)).astype(BF16)


def solution(mesh):
    mesh = Mesh(mesh.devices.reshape(4, 2, 4, 4, 2), ("zh", "zl", "y", "x", "tp"))
    ep = ("zh", "zl", "y", "x")
    in_specs = (
        P(ep, "tp"),
        P("tp"),
        P(ep, None),
        P(ep, None),
        P(ep, None, "tp"),
        P(ep, None, "tp"),
        P(ep, None, "tp"),
    )

    return jax.shard_map(local, mesh=mesh, in_specs=in_specs, out_specs=P(ep, "tp"), check_vma=False)
```

```python
import functools

import jax
import jax.numpy as jnp
from jax import lax
from jax.experimental import pallas as pl
from jax.experimental.pallas import tpu as pltpu
from jax.sharding import Mesh, PartitionSpec as P


CAP = 8
EPS = 1e-06
INFO = 8
F32 = jnp.float32
BF16 = jnp.bfloat16
dot = functools.partial(jnp.dot, preferred_element_type=F32)


def iota(shape, dim):
    return lax.broadcasted_iota(jnp.int32, shape, dim)


def one_hot(mask):
    return mask.astype(F32).astype(BF16)


def parts(value):
    high = value.astype(BF16).astype(F32)
    middle = (value - high).astype(BF16).astype(F32)
    return [high, middle, value - high - middle]


def gather_kernel(own_ref, gain_ref, route_ref, weight_ref, out_ref):
    rows, half = own_ref.shape
    out_ref[0:rows, :] = own_ref[...]
    pad = jnp.zeros((5, half), F32)
    out_ref[rows:, :] = jnp.concatenate(
        [jnp.zeros((INFO, half), F32), *parts(gain_ref[...]), pad], axis=0
    ).astype(BF16)
    info = jnp.concatenate([route_ref[...].astype(F32), *parts(weight_ref[...])], axis=0)
    out_ref[rows : rows + INFO, 0:rows] = info.astype(BF16)


def norm_kernel(held_ref, other_ref, out_ref):
    rows, half = other_ref.shape
    own = held_ref[0:rows, :].astype(F32)
    other = other_ref[...].astype(F32)
    total = jnp.sum(own * own, axis=1, keepdims=True) + jnp.sum(other * other, axis=1, keepdims=True)
    scale = lax.rsqrt(total / (2 * half) + EPS)
    tail = held_ref[rows:, :]
    gain = tail[INFO:, :].astype(F32)
    gain = gain[0:1] + gain[1:2] + gain[2:3]
    out_ref[0:rows, :] = (own * scale * gain).astype(BF16)
    out_ref[rows:, :] = tail[0:INFO, :]


def dispatch_kernel(place_ref, own_ref, first_ref, third_ref, second_ref, out_ref, table0_ref, table1_ref):
    place_pair(0, place_ref, own_ref, first_ref, out_ref, table0_ref)
    place_pair(1, place_ref, third_ref, second_ref, out_ref, table1_ref)


def place_pair(pair, place_ref, a_ref, b_ref, out_ref, table_ref):
    rows = a_ref.shape[0] - INFO
    span = 2 * rows
    peers, block, half = out_ref.shape
    experts = 2 * peers
    earlier = one_hot(
        (iota((span, span), 0) < iota((span, span), 1))
        & (iota((span, span), 0) // rows == iota((span, span), 1) // rows)
    )
    side = iota((1, span), 1) // rows
    expert = iota((experts, span), 0)
    info = jnp.concatenate([a_ref[rows:, 0:rows].astype(F32), b_ref[rows:, 0:rows].astype(F32)], axis=1)
    tokens = jnp.concatenate([a_ref[0:rows, :], b_ref[0:rows, :]], axis=0)
    picks = [info[k : k + 1].astype(jnp.int32) - place_ref[0] // 2 * experts for k in range(2)]
    ahead = dot(one_hot((expert == picks[0]) | (expert == picks[1])), earlier)
    slots, weights = [], []
    for k, pick in enumerate(picks):
        rank = jnp.sum(jnp.where(expert == pick, ahead, 0.0), axis=0, keepdims=True).astype(jnp.int32)
        slot = (pick % 2) * (16 * peers) + (pick // 2) * 16 + side * CAP + rank
        slots.append(jnp.where((pick >= 0) & (pick < experts), slot, -1))
        weights.append(info[2 + k : 3 + k] + info[4 + k : 5 + k] + info[6 + k : 7 + k])
    for local in range(2):
        at = local * (block // 2) + 16 * pair
        slot = iota((16 * peers, span), 0) + local * 16 * peers
        sent = dot(one_hot((slot == slots[0]) | (slot == slots[1])), tokens)
        out_ref[:, at : at + 16, :] = sent.astype(BF16).reshape(peers, 16, half)
    columns = [slot.astype(F32) for slot in slots] + weights
    table_ref[...] = jnp.concatenate(columns + columns, axis=0).T


STEP = 512


def hidden_part(rows_ref, at, gate_ref, up_ref, core):
    _, _, block, half = rows_ref.shape
    low, high = (rows_ref[at : at + STEP // block, side].reshape(STEP, half) for side in range(2))
    gate, up = (dot(low, ref[core, 0:half, :]) + dot(high, ref[core, half:, :]) for ref in (gate_ref, up_ref))
    return (gate / (1.0 + jnp.exp(-gate)) * up).astype(BF16)


def own_kernel(place_ref, rows_ref, gate_ref, up_ref, out_ref):
    chips, _, block, _ = rows_ref.shape
    for at in range(0, chips, STEP // block):
        out_ref[at * block : at * block + STEP] = hidden_part(rows_ref, at, gate_ref, up_ref, place_ref[0] % 2)


def expert_kernel(place_ref, rows_ref, own_ref, gate2_ref, up2_ref, down_ref, down2_ref, out_ref):
    core = place_ref[0] % 2
    chips, _, block, half = rows_ref.shape
    width = own_ref.shape[1]
    sides = (core, 1 - core)
    spans = [pl.ds(pl.multiple_of(side * width, width), width) for side in sides]
    step = STEP // block
    for at in range(0, chips, step):
        own = own_ref[at * block : at * block + STEP]
        other = hidden_part(rows_ref, at, gate2_ref, up2_ref, core)
        for side, down in zip(sides, (down_ref, down2_ref)):
            result = dot(own, down[core, spans[0], :]) + dot(other, down[core, spans[1], :])
            out_ref[at : at + step, side] = result.astype(BF16).reshape(step, block, half)


def combine_kernel(pair, back_ref, table_ref, a_ref, b_ref):
    rows, half = a_ref.shape
    peers, block, _ = back_ref.shape
    picked = [None, None]
    for local in range(2):
        at = local * (block // 2) + 16 * pair
        back = back_ref[:, at : at + 16, :].reshape(16 * peers, half)
        place = iota((2 * rows, 16 * peers), 1) + local * 16 * peers
        for k in range(2):
            term = dot(one_hot(place == table_ref[:, k : k + 1].astype(jnp.int32)), back)
            picked[k] = term if picked[k] is None else picked[k] + term
    total = (picked[0] * table_ref[:, 2:3] + picked[1] * table_ref[:, 3:4]).astype(BF16)
    a_ref[...] = total[0:rows]
    b_ref[...] = total[rows:]


def call(kernel, out_shape, args, flops, grant, scalars=0, **kw):
    moved = sum(a.size * a.dtype.itemsize for a in args)
    smem = pl.BlockSpec(memory_space=pltpu.SMEM)
    whole = pl.BlockSpec(memory_space=pltpu.VMEM)
    kw.setdefault("in_specs", [smem] * scalars + [whole] * (len(args) - scalars))
    return pl.pallas_call(
        kernel,
        out_shape=out_shape,
        cost_estimate=pl.CostEstimate(flops=flops, bytes_accessed=moved, transcendentals=0),
        compiler_params=pltpu.CompilerParams(vmem_limit_bytes=grant << 20),
        **kw,
    )(*args)


def local(tokens, norm_gain, routing, route_weight, w_gate, w_up, w_down):
    rows, half = tokens.shape
    columns = lax.axis_size("zh")
    plane = ("zl", "y", "x", "tp")
    peers = lax.axis_size(plane) // 2
    experts, _, width = w_gate.shape
    block = experts * columns * CAP
    total = peers * block
    place = (lax.axis_index("zh") * 2 + lax.axis_index("tp")).astype(jnp.int32).reshape(1)

    def swap(v):
        return lax.ppermute(v, "tp", [(0, 1), (1, 0)])

    def relay(v, by, home=False):
        planes = lax.axis_size(("zh", "zl"))
        pairs = [(z, (z - by if z % 2 else z + by) % planes) for z in range(planes)]
        return lax.ppermute(v, ("zh", "zl"), [(to, z) for z, to in pairs] if home else pairs)

    def exchange(v, axes):
        return lax.all_to_all(v, axes, split_axis=0, concat_axis=0, tiled=True)

    other = swap(tokens)
    gate2, up2, down2 = swap(w_gate), swap(w_up), swap(w_down)
    held = call(
        gather_kernel,
        jax.ShapeDtypeStruct((rows + INFO + 8, half), BF16),
        (tokens, norm_gain.reshape(1, half), routing.T, route_weight.T),
        rows * half,
        60,
    )
    own = call(norm_kernel, jax.ShapeDtypeStruct((rows + INFO, half), BF16), (held, other), rows * half, 4)
    third = relay(own, -3)
    second, first = relay(own, 2), relay(own, -1)

    buffer = jax.ShapeDtypeStruct((peers, block, half), BF16)
    small = jax.ShapeDtypeStruct((2 * rows, 8), F32)
    flops = total * 2 * rows * half
    sent, table0, table1 = call(
        dispatch_kernel, (buffer, small, small), (place, own, first, third, second), 2 * flops, 12, 1
    )
    arrived = exchange(sent.reshape(2 * peers, block // 2, half), plane)
    arrived = arrived.reshape(peers, 2, block // 2, half)
    hidden = call(
        own_kernel,
        jax.ShapeDtypeStruct((total // 2, width), BF16),
        (place, arrived, w_gate, w_up),
        total * half * width * 4,
        12,
        1,
    )
    result = call(
        expert_kernel,
        jax.ShapeDtypeStruct((peers, 2, block // 2, half), BF16),
        (place, arrived, hidden, gate2, up2, w_down, down2),
        total * half * width * 8,
        16,
        1,
    )
    back = exchange(result.reshape(2 * peers, block // 2, half), plane)
    back = back.reshape(peers, block, half)
    pair = (jax.ShapeDtypeStruct((rows, half), BF16),) * 2
    third, second = call(functools.partial(combine_kernel, 1), pair, (back, table1), 2 * flops, 8)
    home = [relay(third, -3, home=True)]
    own, first = call(functools.partial(combine_kernel, 0), pair, (back, table0), 2 * flops, 8)
    home += [relay(second, 2, home=True), relay(first, -1, home=True)]
    return sum((part.astype(F32) for part in home), own.astype(F32)).astype(BF16)


def solution(mesh):
    mesh = Mesh(mesh.devices.reshape(4, 2, 4, 4, 2), ("zh", "zl", "y", "x", "tp"))
    ep = ("zh", "zl", "y", "x")
    in_specs = (
        P(ep, "tp"),
        P("tp"),
        P(ep, None),
        P(ep, None),
        P(ep, None, "tp"),
        P(ep, None, "tp"),
        P(ep, None, "tp"),
    )

    return jax.shard_map(local, mesh=mesh, in_specs=in_specs, out_specs=P(ep, "tp"), check_vma=False)
```

```python
import functools

import jax
import jax.numpy as jnp
from jax import lax
from jax.experimental import pallas as pl
from jax.experimental.pallas import tpu as pltpu
from jax.sharding import Mesh, PartitionSpec as P


CAP = 8
EPS = 1e-06
INFO = 8
F32 = jnp.float32
BF16 = jnp.bfloat16
dot = functools.partial(jnp.dot, preferred_element_type=F32)


def iota(shape, dim):
    return lax.broadcasted_iota(jnp.int32, shape, dim)


def one_hot(mask):
    return mask.astype(F32).astype(BF16)


def parts(value):
    high = value.astype(BF16).astype(F32)
    middle = (value - high).astype(BF16).astype(F32)
    return [high, middle, value - high - middle]


def gather_kernel(own_ref, gain_ref, route_ref, weight_ref, out_ref):
    rows, half = own_ref.shape
    out_ref[0:rows, :] = own_ref[...]
    pad = jnp.zeros((5, half), F32)
    out_ref[rows:, :] = jnp.concatenate(
        [jnp.zeros((INFO, half), F32), *parts(gain_ref[...]), pad], axis=0
    ).astype(BF16)
    info = jnp.concatenate([route_ref[...].astype(F32), *parts(weight_ref[...])], axis=0)
    out_ref[rows : rows + INFO, 0:rows] = info.astype(BF16)


def norm_kernel(held_ref, other_ref, out_ref):
    rows, half = other_ref.shape
    own = held_ref[0:rows, :].astype(F32)
    other = other_ref[...].astype(F32)
    total = jnp.sum(own * own, axis=1, keepdims=True) + jnp.sum(other * other, axis=1, keepdims=True)
    scale = lax.rsqrt(total / (2 * half) + EPS)
    tail = held_ref[rows:, :]
    gain = tail[INFO:, :].astype(F32)
    gain = gain[0:1] + gain[1:2] + gain[2:3]
    out_ref[0:rows, :] = (own * scale * gain).astype(BF16)
    out_ref[rows:, :] = tail[0:INFO, :]


def dispatch_kernel(place_ref, own_ref, first_ref, third_ref, second_ref, out_ref, table0_ref, table1_ref):
    place_pair(0, place_ref, own_ref, first_ref, out_ref, table0_ref)
    place_pair(1, place_ref, third_ref, second_ref, out_ref, table1_ref)


def place_pair(pair, place_ref, a_ref, b_ref, out_ref, table_ref):
    rows = a_ref.shape[0] - INFO
    span = 2 * rows
    peers, block, half = out_ref.shape
    experts = 2 * peers
    earlier = one_hot(
        (iota((span, span), 0) < iota((span, span), 1))
        & (iota((span, span), 0) // rows == iota((span, span), 1) // rows)
    )
    side = iota((1, span), 1) // rows
    expert = iota((experts, span), 0)
    info = jnp.concatenate([a_ref[rows:, 0:rows].astype(F32), b_ref[rows:, 0:rows].astype(F32)], axis=1)
    tokens = jnp.concatenate([a_ref[0:rows, :], b_ref[0:rows, :]], axis=0)
    picks = [info[k : k + 1].astype(jnp.int32) - place_ref[0] // 2 * experts for k in range(2)]
    ahead = dot(one_hot((expert == picks[0]) | (expert == picks[1])), earlier)
    slots, weights = [], []
    for k, pick in enumerate(picks):
        rank = jnp.sum(jnp.where(expert == pick, ahead, 0.0), axis=0, keepdims=True).astype(jnp.int32)
        slot = (pick % 2) * (16 * peers) + (pick // 2) * 16 + side * CAP + rank
        slots.append(jnp.where((pick >= 0) & (pick < experts), slot, -1))
        weights.append(info[2 + k : 3 + k] + info[4 + k : 5 + k] + info[6 + k : 7 + k])
    for local in range(2):
        at = local * (block // 2) + 16 * pair
        slot = iota((16 * peers, span), 0) + local * 16 * peers
        sent = dot(one_hot((slot == slots[0]) | (slot == slots[1])), tokens)
        out_ref[:, at : at + 16, :] = sent.astype(BF16).reshape(peers, 16, half)
    columns = [slot.astype(F32) for slot in slots] + weights
    table_ref[...] = jnp.concatenate(columns + columns, axis=0).T


STEP = 512


def hidden_part(rows_ref, at, gate_ref, up_ref, core):
    _, _, block, half = rows_ref.shape
    low, high = (rows_ref[at : at + STEP // block, side].reshape(STEP, half) for side in range(2))
    gate, up = (dot(low, ref[core, 0:half, :]) + dot(high, ref[core, half:, :]) for ref in (gate_ref, up_ref))
    return (gate / (1.0 + jnp.exp(-gate)) * up).astype(BF16)


def own_kernel(place_ref, rows_ref, gate_ref, up_ref, out_ref):
    chips, _, block, _ = rows_ref.shape
    for at in range(0, chips, STEP // block):
        out_ref[at * block : at * block + STEP] = hidden_part(rows_ref, at, gate_ref, up_ref, place_ref[0] % 2)


def expert_kernel(place_ref, rows_ref, own_ref, gate2_ref, up2_ref, down_ref, down2_ref, out_ref):
    core = place_ref[0] % 2
    chips, _, block, half = rows_ref.shape
    width = own_ref.shape[1]
    sides = (core, 1 - core)
    spans = [pl.ds(pl.multiple_of(side * width, width), width) for side in sides]
    step = STEP // block
    for at in range(0, chips, step):
        own = own_ref[at * block : at * block + STEP]
        other = hidden_part(rows_ref, at, gate2_ref, up2_ref, core)
        for side, down in zip(sides, (down_ref, down2_ref)):
            result = dot(own, down[core, spans[0], :]) + dot(other, down[core, spans[1], :])
            out_ref[at : at + step, side] = result.astype(BF16).reshape(step, block, half)


def combine_kernel(pair, back_ref, table_ref, a_ref, b_ref):
    rows, half = a_ref.shape
    peers, block, _ = back_ref.shape
    picked = None
    for local in range(2):
        at = local * (block // 2) + 16 * pair
        back = back_ref[:, at : at + 16, :].reshape(16 * peers, half)
        place = iota((2 * rows, 16 * peers), 1) + local * 16 * peers
        chosen = [one_hot(place == table_ref[:, k : k + 1].astype(jnp.int32)) for k in range(2)]
        term = dot(jnp.concatenate(chosen, axis=0), back)
        picked = term if picked is None else picked + term
    total = picked[0 : 2 * rows] * table_ref[:, 2:3] + picked[2 * rows :] * table_ref[:, 3:4]
    total = total.astype(BF16)
    a_ref[...] = total[0:rows]
    b_ref[...] = total[rows:]


def call(kernel, out_shape, args, flops, grant, scalars=0, **kw):
    moved = sum(a.size * a.dtype.itemsize for a in args)
    smem = pl.BlockSpec(memory_space=pltpu.SMEM)
    whole = pl.BlockSpec(memory_space=pltpu.VMEM)
    kw.setdefault("in_specs", [smem] * scalars + [whole] * (len(args) - scalars))
    return pl.pallas_call(
        kernel,
        out_shape=out_shape,
        cost_estimate=pl.CostEstimate(flops=flops, bytes_accessed=moved, transcendentals=0),
        compiler_params=pltpu.CompilerParams(vmem_limit_bytes=grant << 20),
        **kw,
    )(*args)


def local(tokens, norm_gain, routing, route_weight, w_gate, w_up, w_down):
    rows, half = tokens.shape
    columns = lax.axis_size("zh")
    plane = ("zl", "y", "x", "tp")
    peers = lax.axis_size(plane) // 2
    experts, _, width = w_gate.shape
    block = experts * columns * CAP
    total = peers * block
    place = (lax.axis_index("zh") * 2 + lax.axis_index("tp")).astype(jnp.int32).reshape(1)

    def swap(v):
        return lax.ppermute(v, "tp", [(0, 1), (1, 0)])

    def relay(v, by, home=False):
        planes = lax.axis_size(("zh", "zl"))
        pairs = [(z, (z - by if z % 2 else z + by) % planes) for z in range(planes)]
        return lax.ppermute(v, ("zh", "zl"), [(to, z) for z, to in pairs] if home else pairs)

    def exchange(v, axes):
        return lax.all_to_all(v, axes, split_axis=0, concat_axis=0, tiled=True)

    other = swap(tokens)
    gate2, up2, down2 = swap(w_gate), swap(w_up), swap(w_down)
    held = call(
        gather_kernel,
        jax.ShapeDtypeStruct((rows + INFO + 8, half), BF16),
        (tokens, norm_gain.reshape(1, half), routing.T, route_weight.T),
        rows * half,
        60,
    )
    own = call(norm_kernel, jax.ShapeDtypeStruct((rows + INFO, half), BF16), (held, other), rows * half, 4)
    third = relay(own, -3)
    first = relay(own, -1)
    second = relay(own, 2)

    buffer = jax.ShapeDtypeStruct((peers, block, half), BF16)
    small = jax.ShapeDtypeStruct((2 * rows, 8), F32)
    flops = total * 2 * rows * half
    sent, table0, table1 = call(
        dispatch_kernel, (buffer, small, small), (place, own, first, third, second), 2 * flops, 12, 1
    )
    arrived = exchange(sent.reshape(2 * peers, block // 2, half), plane)
    arrived = arrived.reshape(peers, 2, block // 2, half)
    hidden = call(
        own_kernel,
        jax.ShapeDtypeStruct((total // 2, width), BF16),
        (place, arrived, w_gate, w_up),
        total * half * width * 4,
        12,
        1,
    )
    result = call(
        expert_kernel,
        jax.ShapeDtypeStruct((peers, 2, block // 2, half), BF16),
        (place, arrived, hidden, gate2, up2, w_down, down2),
        total * half * width * 8,
        16,
        1,
    )
    back = exchange(result.reshape(2 * peers, block // 2, half), plane)
    back = back.reshape(peers, block, half)
    pair = (jax.ShapeDtypeStruct((rows, half), BF16),) * 2
    third, second = call(functools.partial(combine_kernel, 1), pair, (back, table1), 2 * flops, 8)
    home = [relay(third, -3, home=True)]
    home += [relay(second, 2, home=True)]
    own, first = call(functools.partial(combine_kernel, 0), pair, (back, table0), 2 * flops, 8)
    home += [relay(first, -1, home=True)]
    return sum((part.astype(F32) for part in home), own.astype(F32)).astype(BF16)


def solution(mesh):
    mesh = Mesh(mesh.devices.reshape(4, 2, 4, 4, 2), ("zh", "zl", "y", "x", "tp"))
    ep = ("zh", "zl", "y", "x")
    in_specs = (
        P(ep, "tp"),
        P("tp"),
        P(ep, None),
        P(ep, None),
        P(ep, None, "tp"),
        P(ep, None, "tp"),
        P(ep, None, "tp"),
    )

    return jax.shard_map(local, mesh=mesh, in_specs=in_specs, out_specs=P(ep, "tp"), check_vma=False)
```

```python
import functools

import jax
import jax.numpy as jnp
from jax import lax
from jax.experimental import pallas as pl
from jax.experimental.pallas import tpu as pltpu
from jax.sharding import Mesh, PartitionSpec as P


CAP = 8
EPS = 1e-06
INFO = 8
F32 = jnp.float32
BF16 = jnp.bfloat16
dot = functools.partial(jnp.dot, preferred_element_type=F32)


def iota(shape, dim):
    return lax.broadcasted_iota(jnp.int32, shape, dim)


def one_hot(mask):
    return mask.astype(F32).astype(BF16)


def parts(value):
    high = value.astype(BF16).astype(F32)
    middle = (value - high).astype(BF16).astype(F32)
    return [high, middle, value - high - middle]


def gather_kernel(own_ref, gain_ref, route_ref, weight_ref, out_ref):
    rows, half = own_ref.shape
    out_ref[0:rows, :] = own_ref[...]
    pad = jnp.zeros((5, half), F32)
    out_ref[rows:, :] = jnp.concatenate(
        [jnp.zeros((INFO, half), F32), *parts(gain_ref[...]), pad], axis=0
    ).astype(BF16)
    info = jnp.concatenate([route_ref[...].astype(F32), *parts(weight_ref[...])], axis=0)
    out_ref[rows : rows + INFO, 0:rows] = info.astype(BF16)


def norm_kernel(held_ref, other_ref, out_ref):
    rows, half = other_ref.shape
    own = held_ref[0:rows, :].astype(F32)
    other = other_ref[...].astype(F32)
    total = jnp.sum(own * own, axis=1, keepdims=True) + jnp.sum(other * other, axis=1, keepdims=True)
    scale = lax.rsqrt(total / (2 * half) + EPS)
    tail = held_ref[rows:, :]
    gain = tail[INFO:, :].astype(F32)
    gain = gain[0:1] + gain[1:2] + gain[2:3]
    out_ref[0:rows, :] = (own * scale * gain).astype(BF16)
    out_ref[rows:, :] = tail[0:INFO, :]


def early_kernel(place_ref, own_ref, first_ref, rows_ref, table_ref):
    place_pair(place_ref, own_ref, first_ref, rows_ref, table_ref)


def dispatch_kernel(place_ref, third_ref, second_ref, early_ref, out_ref, table_ref):
    for local in range(2):
        at = local * out_ref.shape[1] // 2
        out_ref[:, at : at + 16, :] = early_ref[:, 16 * local : 16 * (local + 1), :]
    place_pair(place_ref, third_ref, second_ref, out_ref, table_ref, 16)


def place_pair(place_ref, a_ref, b_ref, out_ref, table_ref, start=0):
    rows = a_ref.shape[0] - INFO
    span = 2 * rows
    peers, block, half = out_ref.shape
    experts = 2 * peers
    earlier = one_hot(
        (iota((span, span), 0) < iota((span, span), 1))
        & (iota((span, span), 0) // rows == iota((span, span), 1) // rows)
    )
    side = iota((1, span), 1) // rows
    expert = iota((experts, span), 0)
    info = jnp.concatenate([a_ref[rows:, 0:rows].astype(F32), b_ref[rows:, 0:rows].astype(F32)], axis=1)
    tokens = jnp.concatenate([a_ref[0:rows, :], b_ref[0:rows, :]], axis=0)
    picks = [info[k : k + 1].astype(jnp.int32) - place_ref[0] // 2 * experts for k in range(2)]
    ahead = dot(one_hot((expert == picks[0]) | (expert == picks[1])), earlier)
    slots, weights = [], []
    for k, pick in enumerate(picks):
        rank = jnp.sum(jnp.where(expert == pick, ahead, 0.0), axis=0, keepdims=True).astype(jnp.int32)
        slot = (pick % 2) * (16 * peers) + (pick // 2) * 16 + side * CAP + rank
        slots.append(jnp.where((pick >= 0) & (pick < experts), slot, -1))
        weights.append(info[2 + k : 3 + k] + info[4 + k : 5 + k] + info[6 + k : 7 + k])
    for local in range(2):
        at = local * (block // 2) + start
        slot = iota((16 * peers, span), 0) + local * 16 * peers
        sent = dot(one_hot((slot == slots[0]) | (slot == slots[1])), tokens)
        out_ref[:, at : at + 16, :] = sent.astype(BF16).reshape(peers, 16, half)
    columns = [slot.astype(F32) for slot in slots] + weights
    table_ref[...] = jnp.concatenate(columns + columns, axis=0).T


STEP = 512


def hidden_part(rows_ref, at, gate_ref, up_ref, core):
    _, _, block, half = rows_ref.shape
    low, high = (rows_ref[at : at + STEP // block, side].reshape(STEP, half) for side in range(2))
    gate, up = (dot(low, ref[core, 0:half, :]) + dot(high, ref[core, half:, :]) for ref in (gate_ref, up_ref))
    return (gate / (1.0 + jnp.exp(-gate)) * up).astype(BF16)


def own_kernel(place_ref, rows_ref, gate_ref, up_ref, out_ref):
    chips, _, block, _ = rows_ref.shape
    for at in range(0, chips, STEP // block):
        out_ref[at * block : at * block + STEP] = hidden_part(rows_ref, at, gate_ref, up_ref, place_ref[0] % 2)


def expert_kernel(place_ref, rows_ref, own_ref, gate2_ref, up2_ref, down_ref, down2_ref, out_ref):
    core = place_ref[0] % 2
    chips, _, block, half = rows_ref.shape
    width = own_ref.shape[1]
    sides = (core, 1 - core)
    spans = [pl.ds(pl.multiple_of(side * width, width), width) for side in sides]
    step = STEP // block
    for at in range(0, chips, step):
        own = own_ref[at * block : at * block + STEP]
        other = hidden_part(rows_ref, at, gate2_ref, up2_ref, core)
        for side, down in zip(sides, (down_ref, down2_ref)):
            result = dot(own, down[core, spans[0], :]) + dot(other, down[core, spans[1], :])
            out_ref[at : at + step, side] = result.astype(BF16).reshape(step, block, half)


def combine_kernel(pair, back_ref, table_ref, a_ref, b_ref):
    rows, half = a_ref.shape
    peers, block, _ = back_ref.shape
    picked = None
    for local in range(2):
        at = local * (block // 2) + 16 * pair
        back = back_ref[:, at : at + 16, :].reshape(16 * peers, half)
        place = iota((2 * rows, 16 * peers), 1) + local * 16 * peers
        chosen = [one_hot(place == table_ref[:, k : k + 1].astype(jnp.int32)) for k in range(2)]
        term = dot(jnp.concatenate(chosen, axis=0), back)
        picked = term if picked is None else picked + term
    total = picked[0 : 2 * rows] * table_ref[:, 2:3] + picked[2 * rows :] * table_ref[:, 3:4]
    total = total.astype(BF16)
    a_ref[...] = total[0:rows]
    b_ref[...] = total[rows:]


def call(kernel, out_shape, args, flops, grant, scalars=0, **kw):
    moved = sum(a.size * a.dtype.itemsize for a in args)
    smem = pl.BlockSpec(memory_space=pltpu.SMEM)
    whole = pl.BlockSpec(memory_space=pltpu.VMEM)
    kw.setdefault("in_specs", [smem] * scalars + [whole] * (len(args) - scalars))
    return pl.pallas_call(
        kernel,
        out_shape=out_shape,
        cost_estimate=pl.CostEstimate(flops=flops, bytes_accessed=moved, transcendentals=0),
        compiler_params=pltpu.CompilerParams(vmem_limit_bytes=grant << 20),
        **kw,
    )(*args)


def local(tokens, norm_gain, routing, route_weight, w_gate, w_up, w_down):
    rows, half = tokens.shape
    columns = lax.axis_size("zh")
    plane = ("zl", "y", "x", "tp")
    peers = lax.axis_size(plane) // 2
    experts, _, width = w_gate.shape
    block = experts * columns * CAP
    total = peers * block
    place = (lax.axis_index("zh") * 2 + lax.axis_index("tp")).astype(jnp.int32).reshape(1)

    def swap(v):
        return lax.ppermute(v, "tp", [(0, 1), (1, 0)])

    def relay(v, by, home=False):
        planes = lax.axis_size(("zh", "zl"))
        pairs = [(z, (z - by if z % 2 else z + by) % planes) for z in range(planes)]
        return lax.ppermute(v, ("zh", "zl"), [(to, z) for z, to in pairs] if home else pairs)

    def exchange(v, axes):
        return lax.all_to_all(v, axes, split_axis=0, concat_axis=0, tiled=True)

    other = swap(tokens)
    gate2, up2, down2 = swap(w_gate), swap(w_up), swap(w_down)
    held = call(
        gather_kernel,
        jax.ShapeDtypeStruct((rows + INFO + 8, half), BF16),
        (tokens, norm_gain.reshape(1, half), routing.T, route_weight.T),
        rows * half,
        60,
    )
    own = call(norm_kernel, jax.ShapeDtypeStruct((rows + INFO, half), BF16), (held, other), rows * half, 4)
    third = relay(own, -3)
    first = relay(own, -1)
    second = relay(own, 2)

    buffer = jax.ShapeDtypeStruct((peers, block, half), BF16)
    small = jax.ShapeDtypeStruct((2 * rows, 8), F32)
    flops = total * 2 * rows * half
    early, table0 = call(
        early_kernel,
        (jax.ShapeDtypeStruct((peers, block // 2, half), BF16), small),
        (place, own, first),
        flops,
        8,
        1,
    )
    sent, table1 = call(dispatch_kernel, (buffer, small), (place, third, second, early), flops, 8, 1)
    arrived = exchange(sent.reshape(2 * peers, block // 2, half), plane)
    arrived = arrived.reshape(peers, 2, block // 2, half)
    hidden = call(
        own_kernel,
        jax.ShapeDtypeStruct((total // 2, width), BF16),
        (place, arrived, w_gate, w_up),
        total * half * width * 4,
        12,
        1,
    )
    result = call(
        expert_kernel,
        jax.ShapeDtypeStruct((peers, 2, block // 2, half), BF16),
        (place, arrived, hidden, gate2, up2, w_down, down2),
        total * half * width * 8,
        16,
        1,
    )
    back = exchange(result.reshape(2 * peers, block // 2, half), plane)
    back = back.reshape(peers, block, half)
    pair = (jax.ShapeDtypeStruct((rows, half), BF16),) * 2
    third, second = call(functools.partial(combine_kernel, 1), pair, (back, table1), 2 * flops, 8)
    home = [relay(third, -3, home=True)]
    home += [relay(second, 2, home=True)]
    own, first = call(functools.partial(combine_kernel, 0), pair, (back, table0), 2 * flops, 8)
    home += [relay(first, -1, home=True)]
    return sum((part.astype(F32) for part in home), own.astype(F32)).astype(BF16)


def solution(mesh):
    mesh = Mesh(mesh.devices.reshape(4, 2, 4, 4, 2), ("zh", "zl", "y", "x", "tp"))
    ep = ("zh", "zl", "y", "x")
    in_specs = (
        P(ep, "tp"),
        P("tp"),
        P(ep, None),
        P(ep, None),
        P(ep, None, "tp"),
        P(ep, None, "tp"),
        P(ep, None, "tp"),
    )

    return jax.shard_map(local, mesh=mesh, in_specs=in_specs, out_specs=P(ep, "tp"), check_vma=False)
```

```python
import functools

import jax
import jax.numpy as jnp
from jax import lax
from jax.experimental import pallas as pl
from jax.experimental.pallas import tpu as pltpu
from jax.sharding import Mesh, PartitionSpec as P


CAP = 8
EPS = 1e-06
INFO = 8
F32 = jnp.float32
BF16 = jnp.bfloat16
dot = functools.partial(jnp.dot, preferred_element_type=F32)


def iota(shape, dim):
    return lax.broadcasted_iota(jnp.int32, shape, dim)


def one_hot(mask):
    return mask.astype(F32).astype(BF16)


def parts(value):
    high = value.astype(BF16).astype(F32)
    middle = (value - high).astype(BF16).astype(F32)
    return [high, middle, value - high - middle]


def gather_kernel(own_ref, gain_ref, route_ref, weight_ref, out_ref):
    rows, half = own_ref.shape
    out_ref[0:rows, :] = own_ref[...]
    pad = jnp.zeros((5, half), F32)
    out_ref[rows:, :] = jnp.concatenate(
        [jnp.zeros((INFO, half), F32), *parts(gain_ref[...]), pad], axis=0
    ).astype(BF16)
    info = jnp.concatenate([route_ref[...].astype(F32), *parts(weight_ref[...])], axis=0)
    out_ref[rows : rows + INFO, 0:rows] = info.astype(BF16)


def norm_kernel(held_ref, other_ref, out_ref):
    rows, half = other_ref.shape
    own = held_ref[0:rows, :].astype(F32)
    other = other_ref[...].astype(F32)
    total = jnp.sum(own * own, axis=1, keepdims=True) + jnp.sum(other * other, axis=1, keepdims=True)
    scale = lax.rsqrt(total / (2 * half) + EPS)
    tail = held_ref[rows:, :]
    gain = tail[INFO:, :].astype(F32)
    gain = gain[0:1] + gain[1:2] + gain[2:3]
    out_ref[0:rows, :] = (own * scale * gain).astype(BF16)
    out_ref[rows:, :] = tail[0:INFO, :]


def dispatch_kernel(place_ref, own_ref, first_ref, third_ref, second_ref, out_ref, table0_ref, table1_ref):
    place_pair(0, place_ref, own_ref, first_ref, out_ref, table0_ref)
    place_pair(1, place_ref, third_ref, second_ref, out_ref, table1_ref)


def place_pair(pair, place_ref, a_ref, b_ref, out_ref, table_ref):
    rows = a_ref.shape[0] - INFO
    span = 2 * rows
    _, peers, _, half = out_ref.shape
    experts = 2 * peers
    earlier = one_hot(
        (iota((span, span), 0) < iota((span, span), 1))
        & (iota((span, span), 0) // rows == iota((span, span), 1) // rows)
    )
    side = iota((1, span), 1) // rows
    expert = iota((experts, span), 0)
    info = jnp.concatenate([a_ref[rows:, 0:rows].astype(F32), b_ref[rows:, 0:rows].astype(F32)], axis=1)
    tokens = jnp.concatenate([a_ref[0:rows, :], b_ref[0:rows, :]], axis=0)
    picks = [info[k : k + 1].astype(jnp.int32) - place_ref[0] // 2 * experts for k in range(2)]
    ahead = dot(one_hot((expert == picks[0]) | (expert == picks[1])), earlier)
    slots, weights = [], []
    for k, pick in enumerate(picks):
        rank = jnp.sum(jnp.where(expert == pick, ahead, 0.0), axis=0, keepdims=True).astype(jnp.int32)
        slot = (pick % 2) * (16 * peers) + (pick // 2) * 16 + side * CAP + rank
        slots.append(jnp.where((pick >= 0) & (pick < experts), slot, -1))
        weights.append(info[2 + k : 3 + k] + info[4 + k : 5 + k] + info[6 + k : 7 + k])
    for local in range(2):
        at = 16 * pair
        slot = iota((16 * peers, span), 0) + local * 16 * peers
        sent = dot(one_hot((slot == slots[0]) | (slot == slots[1])), tokens)
        out_ref[local, :, at : at + 16, :] = sent.astype(BF16).reshape(peers, 16, half)
    columns = [slot.astype(F32) for slot in slots] + weights
    table_ref[...] = jnp.concatenate(columns + columns, axis=0).T


STEP = 512


def hidden_part(rows_ref, at, gate_ref, up_ref, core):
    _, _, block, half = rows_ref.shape
    low, high = (rows_ref[side, at : at + STEP // block].reshape(STEP, half) for side in range(2))
    gate, up = (dot(low, ref[core, 0:half, :]) + dot(high, ref[core, half:, :]) for ref in (gate_ref, up_ref))
    return (gate / (1.0 + jnp.exp(-gate)) * up).astype(BF16)


def own_kernel(place_ref, rows_ref, gate_ref, up_ref, out_ref):
    _, chips, block, _ = rows_ref.shape
    for at in range(0, chips, STEP // block):
        out_ref[at * block : at * block + STEP] = hidden_part(rows_ref, at, gate_ref, up_ref, place_ref[0] % 2)


def expert_kernel(place_ref, rows_ref, own_ref, gate2_ref, up2_ref, down_ref, down2_ref, out_ref):
    core = place_ref[0] % 2
    _, chips, block, half = rows_ref.shape
    width = own_ref.shape[1]
    sides = (core, 1 - core)
    spans = [pl.ds(pl.multiple_of(side * width, width), width) for side in sides]
    step = STEP // block
    for at in range(0, chips, step):
        own = own_ref[at * block : at * block + STEP]
        other = hidden_part(rows_ref, at, gate2_ref, up2_ref, core)
        for side, down in zip(sides, (down_ref, down2_ref)):
            result = dot(own, down[core, spans[0], :]) + dot(other, down[core, spans[1], :])
            out_ref[side, at : at + step] = result.astype(BF16).reshape(step, block, half)


def combine_kernel(pair, back_ref, table_ref, a_ref, b_ref):
    rows, half = a_ref.shape
    _, peers, _, _ = back_ref.shape
    picked = None
    for local in range(2):
        at = 16 * pair
        back = back_ref[local, :, at : at + 16, :].reshape(16 * peers, half)
        place = iota((2 * rows, 16 * peers), 1) + local * 16 * peers
        chosen = [one_hot(place == table_ref[:, k : k + 1].astype(jnp.int32)) for k in range(2)]
        term = dot(jnp.concatenate(chosen, axis=0), back)
        picked = term if picked is None else picked + term
    total = picked[0 : 2 * rows] * table_ref[:, 2:3] + picked[2 * rows :] * table_ref[:, 3:4]
    total = total.astype(BF16)
    a_ref[...] = total[0:rows]
    b_ref[...] = total[rows:]


def call(kernel, out_shape, args, flops, grant, scalars=0, **kw):
    moved = sum(a.size * a.dtype.itemsize for a in args)
    smem = pl.BlockSpec(memory_space=pltpu.SMEM)
    whole = pl.BlockSpec(memory_space=pltpu.VMEM)
    kw.setdefault("in_specs", [smem] * scalars + [whole] * (len(args) - scalars))
    return pl.pallas_call(
        kernel,
        out_shape=out_shape,
        cost_estimate=pl.CostEstimate(flops=flops, bytes_accessed=moved, transcendentals=0),
        compiler_params=pltpu.CompilerParams(vmem_limit_bytes=grant << 20),
        **kw,
    )(*args)


def local(tokens, norm_gain, routing, route_weight, w_gate, w_up, w_down):
    rows, half = tokens.shape
    columns = lax.axis_size("zh")
    plane = ("tp", "zl", "y", "x")
    peers = lax.axis_size(plane) // 2
    experts, _, width = w_gate.shape
    block = experts * columns * CAP
    total = peers * block
    place = (lax.axis_index("zh") * 2 + lax.axis_index("tp")).astype(jnp.int32).reshape(1)

    def swap(v):
        return lax.ppermute(v, "tp", [(0, 1), (1, 0)])

    def relay(v, by, home=False):
        planes = lax.axis_size(("zh", "zl"))
        pairs = [(z, (z - by if z % 2 else z + by) % planes) for z in range(planes)]
        return lax.ppermute(v, ("zh", "zl"), [(to, z) for z, to in pairs] if home else pairs)

    def exchange(v, axes):
        return lax.all_to_all(v, axes, split_axis=0, concat_axis=0, tiled=True)

    other = swap(tokens)
    gate2, up2, down2 = swap(w_gate), swap(w_up), swap(w_down)
    held = call(
        gather_kernel,
        jax.ShapeDtypeStruct((rows + INFO + 8, half), BF16),
        (tokens, norm_gain.reshape(1, half), routing.T, route_weight.T),
        rows * half,
        60,
    )
    own = call(norm_kernel, jax.ShapeDtypeStruct((rows + INFO, half), BF16), (held, other), rows * half, 4)
    third = relay(own, -3)
    first = relay(own, -1)
    second = relay(own, 2)

    buffer = jax.ShapeDtypeStruct((2, peers, block // 2, half), BF16)
    small = jax.ShapeDtypeStruct((2 * rows, 8), F32)
    flops = total * 2 * rows * half
    sent, table0, table1 = call(
        dispatch_kernel, (buffer, small, small), (place, own, first, third, second), 2 * flops, 12, 1
    )
    arrived = exchange(sent.reshape(2 * peers, block // 2, half), plane)
    arrived = arrived.reshape(2, peers, block // 2, half)
    hidden = call(
        own_kernel,
        jax.ShapeDtypeStruct((total // 2, width), BF16),
        (place, arrived, w_gate, w_up),
        total * half * width * 4,
        12,
        1,
    )
    result = call(
        expert_kernel,
        buffer,
        (place, arrived, hidden, gate2, up2, w_down, down2),
        total * half * width * 8,
        16,
        1,
    )
    back = exchange(result.reshape(2 * peers, block // 2, half), plane)
    back = back.reshape(2, peers, block // 2, half)
    pair = (jax.ShapeDtypeStruct((rows, half), BF16),) * 2
    third, second = call(functools.partial(combine_kernel, 1), pair, (back, table1), 2 * flops, 8)
    home = [relay(third, -3, home=True)]
    home += [relay(second, 2, home=True)]
    own, first = call(functools.partial(combine_kernel, 0), pair, (back, table0), 2 * flops, 8)
    home += [relay(first, -1, home=True)]
    return sum((part.astype(F32) for part in home), own.astype(F32)).astype(BF16)


def solution(mesh):
    mesh = Mesh(mesh.devices.reshape(4, 2, 4, 4, 2), ("zh", "zl", "y", "x", "tp"))
    ep = ("zh", "zl", "y", "x")
    in_specs = (
        P(ep, "tp"),
        P("tp"),
        P(ep, None),
        P(ep, None),
        P(ep, None, "tp"),
        P(ep, None, "tp"),
        P(ep, None, "tp"),
    )

    return jax.shard_map(local, mesh=mesh, in_specs=in_specs, out_specs=P(ep, "tp"), check_vma=False)
```

```python
import functools

import jax
import jax.numpy as jnp
from jax import lax
from jax.experimental import pallas as pl
from jax.experimental.pallas import tpu as pltpu
from jax.sharding import Mesh, PartitionSpec as P


CAP = 8
EPS = 1e-06
INFO = 8
F32 = jnp.float32
BF16 = jnp.bfloat16
dot = functools.partial(jnp.dot, preferred_element_type=F32)


def iota(shape, dim):
    return lax.broadcasted_iota(jnp.int32, shape, dim)


def one_hot(mask):
    return mask.astype(F32).astype(BF16)


def parts(value):
    high = value.astype(BF16).astype(F32)
    middle = (value - high).astype(BF16).astype(F32)
    return [high, middle, value - high - middle]


def gather_kernel(own_ref, gain_ref, route_ref, weight_ref, out_ref):
    rows, half = own_ref.shape
    out_ref[0:rows, :] = own_ref[...]
    pad = jnp.zeros((5, half), F32)
    out_ref[rows:, :] = jnp.concatenate(
        [jnp.zeros((INFO, half), F32), *parts(gain_ref[...]), pad], axis=0
    ).astype(BF16)
    info = jnp.concatenate([route_ref[...].astype(F32), *parts(weight_ref[...])], axis=0)
    out_ref[rows : rows + INFO, 0:rows] = info.astype(BF16)


def norm_kernel(held_ref, other_ref, out_ref):
    rows, half = other_ref.shape
    own = held_ref[0:rows, :].astype(F32)
    other = other_ref[...].astype(F32)
    total = jnp.sum(own * own, axis=1, keepdims=True) + jnp.sum(other * other, axis=1, keepdims=True)
    scale = lax.rsqrt(total / (2 * half) + EPS)
    tail = held_ref[rows:, :]
    gain = tail[INFO:, :].astype(F32)
    gain = gain[0:1] + gain[1:2] + gain[2:3]
    out_ref[0:rows, :] = (own * scale * gain).astype(BF16)
    out_ref[rows:, :] = tail[0:INFO, :]


def early_kernel(place_ref, own_ref, first_ref, rows_ref, table_ref):
    place_pair(place_ref, own_ref, first_ref, rows_ref, table_ref)


def dispatch_kernel(place_ref, third_ref, second_ref, early_ref, out_ref, table_ref):
    for local in range(2):
        at = local * out_ref.shape[1] // 2
        out_ref[:, at : at + 16, :] = early_ref[:, 16 * local : 16 * (local + 1), :]
    place_pair(place_ref, third_ref, second_ref, out_ref, table_ref, 16)


def place_pair(place_ref, a_ref, b_ref, out_ref, table_ref, start=0):
    rows = a_ref.shape[0] - INFO
    span = 2 * rows
    peers, block, half = out_ref.shape
    experts = 2 * peers
    earlier = one_hot(
        (iota((span, span), 0) < iota((span, span), 1))
        & (iota((span, span), 0) // rows == iota((span, span), 1) // rows)
    )
    side = iota((1, span), 1) // rows
    expert = iota((experts, span), 0)
    info = jnp.concatenate([a_ref[rows:, 0:rows].astype(F32), b_ref[rows:, 0:rows].astype(F32)], axis=1)
    tokens = jnp.concatenate([a_ref[0:rows, :], b_ref[0:rows, :]], axis=0)
    picks = [info[k : k + 1].astype(jnp.int32) - place_ref[0] // 2 * experts for k in range(2)]
    ahead = dot(one_hot((expert == picks[0]) | (expert == picks[1])), earlier)
    slots, weights = [], []
    for k, pick in enumerate(picks):
        rank = jnp.sum(jnp.where(expert == pick, ahead, 0.0), axis=0, keepdims=True).astype(jnp.int32)
        slot = (pick % 2) * (16 * peers) + (pick // 2) * 16 + side * CAP + rank
        slots.append(jnp.where((pick >= 0) & (pick < experts), slot, -1))
        weights.append(info[2 + k : 3 + k] + info[4 + k : 5 + k] + info[6 + k : 7 + k])
    for local in range(2):
        at = local * (block // 2) + start
        slot = iota((16 * peers, span), 0) + local * 16 * peers
        sent = dot(one_hot((slot == slots[0]) | (slot == slots[1])), tokens)
        out_ref[:, at : at + 16, :] = sent.astype(BF16).reshape(peers, 16, half)
    columns = [slot.astype(F32) for slot in slots] + weights
    table_ref[...] = jnp.concatenate(columns + columns, axis=0).T


STEP = 512


def hidden_part(rows_ref, at, gate_ref, up_ref, core):
    _, _, block, half = rows_ref.shape
    low, high = (rows_ref[at : at + STEP // block, side].reshape(STEP, half) for side in range(2))
    gate, up = (dot(low, ref[core, 0:half, :]) + dot(high, ref[core, half:, :]) for ref in (gate_ref, up_ref))
    return (gate / (1.0 + jnp.exp(-gate)) * up).astype(BF16)


def own_kernel(place_ref, rows_ref, gate_ref, up_ref, out_ref):
    chips, _, block, _ = rows_ref.shape
    for at in range(0, chips, STEP // block):
        out_ref[at * block : at * block + STEP] = hidden_part(rows_ref, at, gate_ref, up_ref, place_ref[0] % 2)


def expert_kernel(place_ref, rows_ref, own_ref, gate2_ref, up2_ref, down_ref, down2_ref, out_ref):
    core = place_ref[0] % 2
    chips, _, block, half = rows_ref.shape
    width = own_ref.shape[1]
    sides = (core, 1 - core)
    spans = [pl.ds(pl.multiple_of(side * width, width), width) for side in sides]
    step = STEP // block
    for at in range(0, chips, step):
        own = own_ref[at * block : at * block + STEP]
        other = hidden_part(rows_ref, at, gate2_ref, up2_ref, core)
        for side, down in zip(sides, (down_ref, down2_ref)):
            result = dot(own, down[core, spans[0], :]) + dot(other, down[core, spans[1], :])
            out_ref[at : at + step, side] = result.astype(BF16).reshape(step, block, half)


def combine_kernel(pair, side, back_ref, table_ref, *out_refs):
    rows, half = out_refs[0].shape
    peers, block, _ = back_ref.shape
    span = rows * len(out_refs)
    table = table_ref[side * rows : side * rows + span, :]
    picked = None
    for local in range(2):
        at = local * (block // 2) + 16 * pair
        back = back_ref[:, at : at + 16, :].reshape(16 * peers, half)
        place = iota((span, 16 * peers), 1) + local * 16 * peers
        chosen = [one_hot(place == table[:, k : k + 1].astype(jnp.int32)) for k in range(2)]
        term = dot(jnp.concatenate(chosen, axis=0), back)
        picked = term if picked is None else picked + term
    total = (picked[0:span] * table[:, 2:3] + picked[span:] * table[:, 3:4]).astype(BF16)
    for i, out_ref in enumerate(out_refs):
        out_ref[...] = total[i * rows : (i + 1) * rows]


def call(kernel, out_shape, args, flops, grant, scalars=0, **kw):
    moved = sum(a.size * a.dtype.itemsize for a in args)
    smem = pl.BlockSpec(memory_space=pltpu.SMEM)
    whole = pl.BlockSpec(memory_space=pltpu.VMEM)
    kw.setdefault("in_specs", [smem] * scalars + [whole] * (len(args) - scalars))
    return pl.pallas_call(
        kernel,
        out_shape=out_shape,
        cost_estimate=pl.CostEstimate(flops=flops, bytes_accessed=moved, transcendentals=0),
        compiler_params=pltpu.CompilerParams(vmem_limit_bytes=grant << 20),
        **kw,
    )(*args)


def local(tokens, norm_gain, routing, route_weight, w_gate, w_up, w_down):
    rows, half = tokens.shape
    columns = lax.axis_size("zh")
    plane = ("zl", "y", "x", "tp")
    peers = lax.axis_size(plane) // 2
    experts, _, width = w_gate.shape
    block = experts * columns * CAP
    total = peers * block
    place = (lax.axis_index("zh") * 2 + lax.axis_index("tp")).astype(jnp.int32).reshape(1)

    def swap(v):
        return lax.ppermute(v, "tp", [(0, 1), (1, 0)])

    def relay(v, by, home=False):
        planes = lax.axis_size(("zh", "zl"))
        pairs = [(z, (z - by if z % 2 else z + by) % planes) for z in range(planes)]
        return lax.ppermute(v, ("zh", "zl"), [(to, z) for z, to in pairs] if home else pairs)

    def exchange(v, axes):
        return lax.all_to_all(v, axes, split_axis=0, concat_axis=0, tiled=True)

    other = swap(tokens)
    gate2, up2, down2 = swap(w_gate), swap(w_up), swap(w_down)
    held = call(
        gather_kernel,
        jax.ShapeDtypeStruct((rows + INFO + 8, half), BF16),
        (tokens, norm_gain.reshape(1, half), routing.T, route_weight.T),
        rows * half,
        60,
    )
    own = call(norm_kernel, jax.ShapeDtypeStruct((rows + INFO, half), BF16), (held, other), rows * half, 4)
    third = relay(own, -3)
    first = relay(own, -1)
    second = relay(own, 2)

    buffer = jax.ShapeDtypeStruct((peers, block, half), BF16)
    small = jax.ShapeDtypeStruct((2 * rows, 8), F32)
    flops = total * 2 * rows * half
    early, table0 = call(
        early_kernel,
        (jax.ShapeDtypeStruct((peers, block // 2, half), BF16), small),
        (place, own, first),
        flops,
        8,
        1,
    )
    sent, table1 = call(dispatch_kernel, (buffer, small), (place, third, second, early), flops, 8, 1)
    arrived = exchange(sent.reshape(2 * peers, block // 2, half), plane)
    arrived = arrived.reshape(peers, 2, block // 2, half)
    hidden = call(
        own_kernel,
        jax.ShapeDtypeStruct((total // 2, width), BF16),
        (place, arrived, w_gate, w_up),
        total * half * width * 4,
        12,
        1,
    )
    result = call(
        expert_kernel,
        jax.ShapeDtypeStruct((peers, 2, block // 2, half), BF16),
        (place, arrived, hidden, gate2, up2, w_down, down2),
        total * half * width * 8,
        16,
        1,
    )
    back = exchange(result.reshape(2 * peers, block // 2, half), plane)
    back = back.reshape(peers, block, half)
    one = jax.ShapeDtypeStruct((rows, half), BF16)
    third = call(functools.partial(combine_kernel, 1, 0), one, (back, table1), flops, 8)
    home = [relay(third, -3, home=True)]
    second = call(functools.partial(combine_kernel, 1, 1), one, (back, table1), flops, 8)
    home += [relay(second, 2, home=True)]
    own, first = call(functools.partial(combine_kernel, 0, 0), (one, one), (back, table0), 2 * flops, 8)
    home += [relay(first, -1, home=True)]
    return sum((part.astype(F32) for part in home), own.astype(F32)).astype(BF16)


def solution(mesh):
    mesh = Mesh(mesh.devices.reshape(4, 2, 4, 4, 2), ("zh", "zl", "y", "x", "tp"))
    ep = ("zh", "zl", "y", "x")
    in_specs = (
        P(ep, "tp"),
        P("tp"),
        P(ep, None),
        P(ep, None),
        P(ep, None, "tp"),
        P(ep, None, "tp"),
        P(ep, None, "tp"),
    )

    return jax.shard_map(local, mesh=mesh, in_specs=in_specs, out_specs=P(ep, "tp"), check_vma=False)
```
